32 devices in a mesh: grp: 2 (over y), ep: 4 (over z), tp: 4 (over x, core).
Axes of the slice: x: 2, y: 2, z: 4, core: 2. Of those that a mesh axis runs over, the one named last changes fastest.
Arguments:
- queries: bfloat16 [3072, 1024], P(('grp', 'ep'), 'tp'), parts along dimension 0, may hold values from -6 to 6
- key_values: bfloat16 [3072, 512], P(('grp', 'ep'), 'tp'), parts along dimension 0, may hold values from -6 to 6
- query_gain: float32 [64], replicated, may hold values from 0.5 to 5
- key_gain: float32 [64], replicated, may hold values from 0.5 to 5
- out_weight: bfloat16 [1024, 2048], P('tp'), may hold values from -0.1875 to 0.1875
- second_batch: bfloat16 [4096, 2048], P(('grp', 'ep', 'tp')), parts along dimension 0, may hold values from -6 to 6
- norm_gain: float32 [2048], replicated, may hold values from 0.1 to 1.9
- routes: int32 [4096, 2], P(('grp', 'ep', 'tp')), parts along dimension 0, may hold values from 0 to 7, all different within a row; in each aligned block of 128 rows (0 to 127, 128 to 255, ...) at most 48 rows name the same one
- route_weights: float32 [4096, 2], P(('grp', 'ep', 'tp')), parts along dimension 0, may hold values from 0.2 to 1
- expert_gate: bfloat16 [8, 2048, 1024], P('ep', None, 'tp'), may hold values from -0.125 to 0.125
- expert_up: bfloat16 [8, 2048, 1024], P('ep', None, 'tp'), may hold values from -0.125 to 0.125
- expert_down: bfloat16 [8, 1024, 2048], P('ep', 'tp'), may hold values from -0.1875 to 0.1875
- shared_gate: bfloat16 [2048, 512], P(None, 'tp'), may hold values from -0.125 to 0.125
- shared_up: bfloat16 [2048, 512], P(None, 'tp'), may hold values from -0.125 to 0.125
- shared_down: bfloat16 [512, 2048], P('tp'), may hold values from -0.25 to 0.25
Outputs:
- mixer_out: bfloat16 [3072, 2048], P(('grp', 'ep', 'tp')), parts along dimension 0
- channel_out: bfloat16 [4096, 2048], P(('grp', 'ep', 'tp')), parts along dimension 0
The draws below stay inside these ranges and needn't reach their ends.
There are 2 independent parts, one for each index of `grp`. The reference program is written for one: setup_inputs(seed, part) draws one part's arguments, and reference() takes and returns one part's arrays. A program takes and returns all parts, laid end to end along the dimension named above; an argument that names none is the same for every part. Nothing has to cross between parts.
Inputs may be any that keep to these rules, and one draw needn't show every extreme that they name: `routes`: each row names 2 different experts. Among the rows of one device no expert is named more than 48 times, and in every draw some expert is named exactly 48 times by the rows of some device.
All inputs are finite; a program needn't handle non-finite values.
Results may differ from the reference program's by a relative error of at most 0.015.
The reference program's roundings to bfloat16 on the way count: a program that leaves them out, or rounds other values in their place, can miss the bound.
Values may be sent and summed in bfloat16 or wider, within the bound.
A program may use at most 128 MiB of HBM per device.

```python
import math
import jax
import jax.numpy as jnp
import numpy as np
from jax import lax

D = 2048
HEAD = 64
HQ_DEV = 4
HQ = 16
KV_HEADS = 4
GRID_W = 64
TOK_A = 384
TOKENS_A = 1536
TOK_B = 128
TOKENS_B = 2048
TOP_K = 2
EXPERTS = 8
FE_DEV = 256
EXPERT_HIDDEN = 1024
SH_DEV = 128
SHARED = 512
CAP = 48
N_EP = 4


def draw_base(key):
    keyvals = jnp.clip(jax.random.normal(jax.random.fold_in(key, 71), (TOKENS_A, KV_HEADS, 2 * HEAD), jnp.float32), -6.0, 6.0)
    queries = jnp.clip(jax.random.normal(jax.random.fold_in(key, 72), (TOKENS_A, HQ, HEAD), jnp.float32), -6.0, 6.0)
    return (queries.reshape(TOKENS_A, HQ * HEAD), keyvals.reshape(TOKENS_A, KV_HEADS * 2 * HEAD))


def draw_queries(key, part):
    return draw_base(key)[0].astype(jnp.bfloat16)


def draw_key_values(key, part):
    return draw_base(key)[1].astype(jnp.bfloat16)


def draw_gain_common(key, salt):
    return 1.0 + 0.18 * jnp.clip(jax.random.normal(jax.random.fold_in(key, salt + 1), (HEAD,), jnp.float32), -2.5, 2.5)


def draw_query_gain(key, part):
    return draw_gain_common(key, 81)


def draw_key_gain(key, part):
    return draw_gain_common(key, 91)


def block_scale(own_key, dims, pieces, low, top_value):
    def one(axis_at, shards_of):
        heights = jax.random.uniform(jax.random.fold_in(jax.random.fold_in(own_key, 6), axis_at), (shards_of,), jnp.float32, low / len(pieces), top_value / len(pieces))
        return jnp.repeat(jnp.exp(heights), dims[axis_at] // shards_of).reshape((-1,) + (1,) * (len(dims) - axis_at - 1))

    level = one(*pieces[0])
    for cut in pieces[1:]:
        level = level * one(*cut)
    return level


def assign_block(rng, own, number, rows, amount, top, reach, slope):
    ranking = jax.random.permutation(rng, amount)
    packed, ordinary = shares(amount, rows * top, reach, slope, True), shares(amount, rows * top, reach, slope, False)
    places = jnp.arange(amount)

    def named(lengths, rotation):
        used = int((lengths > 0).sum())
        fixed = max(1, used // 4)
        passed = fixed + (places - fixed + rotation * (used - fixed)) % max(1, amount - fixed)
        return jnp.zeros((amount,), jnp.int32).at[ranking[jnp.where(places < fixed, places, passed)]].set(jnp.asarray(lengths, jnp.int32))

    lengths = jnp.where(number % 4 == 0, named(packed, number // 4), named(ordinary, number - number // 4 - 1))
    mixed = jax.random.permutation(jax.random.fold_in(own, 3), amount)
    source_of, sink = mixed[0:amount // 2 * 2:2], mixed[1:amount // 2 * 2:2]
    room = jnp.minimum(lengths[source_of] - 1, reach - lengths[sink]) // 2
    room = jnp.where((source_of == ranking[0]) | (sink == ranking[0]) | (lengths[sink] == 0), 0, jnp.maximum(room, 0))
    passed = jax.random.randint(jax.random.fold_in(own, 4), (amount // 2,), 0, 1 << 20) % (room + 1)
    lengths = lengths.at[source_of].add(-passed).at[sink].add(passed)
    items = jnp.searchsorted(jnp.cumsum(lengths), jnp.arange(rows * top), side="right").astype(jnp.int32)
    grid = items.reshape(top, rows).T
    grid = grid[jax.random.permutation(jax.random.fold_in(own, 1), rows)]
    rotation = jax.random.randint(jax.random.fold_in(own, 2), (rows, 1), 0, top)
    return jnp.take_along_axis(grid, (jnp.arange(top)[None, :] + rotation) % top, axis=1)


def shares(amount, total, bound, skew, full):
    loads = [(1 << 20) // math.isqrt(rank ** skew) + 1 for rank in range(1, amount + 1)]
    largest = bound if full else min(bound, max(-(-total // amount), total * loads[0] // sum(loads)))
    least = 1 if total - largest >= amount - 1 else 0
    holding, surplus = [largest] + [least] * (amount - 1), total - largest - least * (amount - 1)
    while surplus > 0:
        candidates = [i for i in range(1, amount) if holding[i] < largest] or [i for i in range(1, amount) if holding[i] < bound]
        mass, budget = sum([loads[i] for i in candidates]), surplus
        for i in candidates:
            extra = min(bound - holding[i], max(1, budget * loads[i] // mass), surplus)
            holding[i] = holding[i] + extra
            surplus = surplus - extra
    return np.array(holding)


def centred(key, extent, width, bound, split=(), held_as=jnp.bfloat16):
    factor_of = block_scale(key, extent, split, -0.22, 0.18) if split else 1.0
    entries = jax.random.normal(key, extent, jnp.float32) * width * factor_of
    return jnp.minimum(jnp.maximum(entries, -bound), bound).astype(held_as)


def setup_inputs(seed: int = 0, part: int = 0) -> dict:
    arg_keys = jax.random.split(jax.random.key(seed), 16)
    own_keys = jax.random.split(jax.random.fold_in(arg_keys[15], part), 16)
    queries = draw_queries(jax.random.fold_in(jax.random.fold_in(arg_keys[15], part), 71), part)
    key_values = draw_key_values(jax.random.fold_in(jax.random.fold_in(arg_keys[15], part), 71), part)
    query_gain = draw_query_gain(jax.random.fold_in(arg_keys[15], 71), part)
    key_gain = draw_key_gain(jax.random.fold_in(arg_keys[15], 71), part)
    out_weight = centred(arg_keys[4], (HQ * HEAD, D), (HQ * HEAD) ** -0.5, 0.1875, ((0, 4),))
    second_batch = centred(own_keys[5], (TOKENS_B, D), 1.0, 6.0, ((0, 16),))
    norm_gain = jnp.clip(1.0 + 0.18 * jax.random.normal(arg_keys[6], (D,), jnp.float32), 0.1, 1.9)
    routes_keys = jax.random.split(jax.random.fold_in(own_keys[7], 1), TOKENS_B // TOK_B)
    routes_turns = jax.random.permutation(jax.random.fold_in(own_keys[7], 3), TOKENS_B // TOK_B)
    routes = jax.vmap(lambda own, number: assign_block(jax.random.fold_in(own_keys[7], 2), own, number, TOK_B, EXPERTS, TOP_K, CAP, 2))(routes_keys, routes_turns).reshape((TOKENS_B, TOP_K))
    route_weights = jnp.clip(0.2 + 0.8 * jax.random.uniform(own_keys[8], (TOKENS_B, TOP_K), jnp.float32) ** block_scale(own_keys[8], (TOKENS_B, TOP_K), ((0, 16),), -0.2, 0.2), 0.2, 1.0)
    expert_gate = centred(arg_keys[9], (EXPERTS, D, EXPERT_HIDDEN), D ** -0.5, 0.125, ((0, 4), (2, 4)))
    expert_up = centred(arg_keys[10], (EXPERTS, D, EXPERT_HIDDEN), D ** -0.5, 0.125, ((0, 4), (2, 4)))
    expert_down = centred(arg_keys[11], (EXPERTS, EXPERT_HIDDEN, D), EXPERT_HIDDEN ** -0.5, 0.1875, ((0, 4), (1, 4)))
    shared_gate = centred(arg_keys[12], (D, SHARED), D ** -0.5, 0.125, ((1, 4),))
    shared_up = centred(arg_keys[13], (D, SHARED), D ** -0.5, 0.125, ((1, 4),))
    shared_down = centred(arg_keys[14], (SHARED, D), SHARED ** -0.5, 0.25, ((0, 4),))
    return dict(queries=queries, key_values=key_values, query_gain=query_gain, key_gain=key_gain, out_weight=out_weight, second_batch=second_batch, norm_gain=norm_gain, routes=routes, route_weights=route_weights, expert_gate=expert_gate, expert_up=expert_up, expert_down=expert_down, shared_gate=shared_gate, shared_up=shared_up, shared_down=shared_down)


rope_base = 10000.0
norm_eps = 1e-06

def head_norm(vectors, gain):
    return vectors * lax.rsqrt(lax.optimization_barrier(jnp.mean(vectors * vectors, axis=-1, keepdims=True)) + norm_eps) * gain

def turn_heads(vectors, positions):
    row_count, head_count, head_size = vectors.shape
    half_size = head_size // 2
    inverse = rope_base ** (-jnp.arange(0, half_size, 2, dtype=jnp.float32) / half_size)
    grid_row = (positions // GRID_W).astype(jnp.float32)
    grid_column = (positions % GRID_W).astype(jnp.float32)
    angles = jnp.concatenate([grid_row[:, None] * inverse, grid_column[:, None] * inverse], axis=-1)
    cosine = jnp.cos(angles)[:, None, :]
    sine = jnp.sin(angles)[:, None, :]
    paired = vectors.reshape(row_count, head_count, half_size, 2)
    first = paired[..., 0]
    second = paired[..., 1]
    turned = jnp.stack([first * cosine - second * sine, first * sine + second * cosine], axis=-1)
    return turned.reshape(vectors.shape)

def slot_ids(route_rows, expert_count, capacity):
    row_count, top_count = route_rows.shape
    flat_routes = route_rows.reshape(-1)
    onehot = (flat_routes[:, None] == jnp.arange(expert_count, dtype=jnp.int32)[None, :]).astype(jnp.int32)
    earlier = (jnp.cumsum(onehot, axis=0).astype(jnp.int32) - onehot).astype(jnp.int32)
    within = lax.optimization_barrier(jnp.sum(earlier * onehot, axis=1)).astype(jnp.int32)
    return (flat_routes * capacity + within).astype(jnp.int32).reshape(row_count, top_count)

def slot_table(slots, slot_count):
    row_count, top_count = slots.shape
    flat_slots = slots.reshape(-1)
    owner_row = jnp.arange(row_count * top_count, dtype=jnp.int32) // top_count
    matches = flat_slots[None, :] == jnp.arange(slot_count, dtype=jnp.int32)[:, None]
    occupied = jnp.any(matches, axis=1)
    source_row = lax.optimization_barrier(jnp.sum(jnp.where(matches, owner_row[None, :], 0), axis=1)).astype(jnp.int32)
    return jnp.where(occupied, source_row, row_count).astype(jnp.int32)

def block_sum(hidden, down_weights, block_width):
    summed = jnp.zeros((hidden.shape[0], down_weights.shape[1]), jnp.float32)
    for block_index in range(hidden.shape[1] // block_width):
        lower = block_index * block_width
        partial_value = jnp.dot(hidden[:, lower:lower + block_width], down_weights[lower:lower + block_width], preferred_element_type=jnp.float32).astype(jnp.bfloat16)
        summed = summed + lax.optimization_barrier(partial_value).astype(jnp.float32)
    return summed

def swiglu_hidden(token_rows, gate_weights, up_weights):
    gate_part = jnp.dot(token_rows, gate_weights, preferred_element_type=jnp.float32)
    up_part = jnp.dot(token_rows, up_weights, preferred_element_type=jnp.float32)
    return (jax.nn.silu(gate_part) * up_part).astype(jnp.bfloat16)

def expert_apply(operands):
    slot_rows, gate_weights, up_weights, down_weights = operands
    hidden = swiglu_hidden(slot_rows, gate_weights, up_weights)
    return block_sum(hidden, down_weights, FE_DEV).astype(jnp.bfloat16)

def reference(queries, key_values, query_gain, key_gain, out_weight, second_batch, norm_gain, routes, route_weights, expert_gate, expert_up, expert_down, shared_gate, shared_up, shared_down):
    total_rows = queries.shape[0]
    positions = jnp.arange(total_rows, dtype=jnp.int32)
    query_turned = turn_heads(head_norm(queries.reshape(total_rows, HQ, HEAD).astype(jnp.float32), query_gain), positions).astype(jnp.bfloat16)
    query_turned = lax.optimization_barrier(query_turned)
    pairs = key_values.reshape(total_rows, KV_HEADS, 2 * HEAD)
    key_turned = turn_heads(head_norm(pairs[:, :, :HEAD].astype(jnp.float32), key_gain), positions).astype(jnp.bfloat16)
    key_float = lax.optimization_barrier(key_turned).astype(jnp.float32)
    value_float = pairs[:, :, HEAD:].astype(jnp.float32)
    scale = HEAD ** (-0.5)

    def query_block(block_queries):
        summed = jnp.zeros((block_queries.shape[0], D), jnp.float32)
        for head_group in range(KV_HEADS):
            group_queries = block_queries[:, head_group * HQ_DEV:(head_group + 1) * HQ_DEV].astype(jnp.float32)
            scores = jnp.einsum('qhd,kd->hqk', group_queries, key_float[:, head_group]) * scale
            top = lax.optimization_barrier(jnp.max(scores, axis=-1, keepdims=True))
            exps = jnp.exp(scores - top)
            totals = lax.optimization_barrier(jnp.sum(exps, axis=-1))
            weights = lax.optimization_barrier(exps.astype(jnp.bfloat16)).astype(jnp.float32)
            numerators = jnp.einsum('hqk,kd->qhd', weights, value_float[:, head_group])
            head_out = (numerators / totals.T[:, :, None]).astype(jnp.bfloat16).reshape(-1, HQ_DEV * HEAD)
            lower = head_group * HQ_DEV * HEAD
            partial_value = jnp.dot(head_out, out_weight[lower:lower + HQ_DEV * HEAD], preferred_element_type=jnp.float32).astype(jnp.bfloat16)
            summed = summed + lax.optimization_barrier(partial_value).astype(jnp.float32)
        return summed.astype(jnp.bfloat16)
    mixer_out = lax.map(query_block, query_turned.reshape(N_EP, TOK_A, HQ, HEAD)).reshape(total_rows, D)
    token_float = second_batch.astype(jnp.float32)
    normed = (token_float * lax.rsqrt(lax.optimization_barrier(jnp.mean(token_float * token_float, axis=-1, keepdims=True)) + norm_eps) * norm_gain).astype(jnp.bfloat16)
    block_count = normed.shape[0] // TOK_B
    slot_count = EXPERTS * CAP
    slots = jax.vmap(lambda route_rows: slot_ids(route_rows, EXPERTS, CAP))(routes.reshape(block_count, TOK_B, TOP_K))
    tables = jax.vmap(lambda slot_block: slot_table(slot_block, slot_count))(slots)
    inputs = jax.vmap(lambda token_rows, table_rows: jnp.take(token_rows, table_rows, axis=0, mode='fill', fill_value=0))(normed.reshape(block_count, TOK_B, D), tables)
    per_expert = inputs.reshape(block_count, EXPERTS, CAP, D).transpose(1, 0, 2, 3).reshape(EXPERTS, block_count * CAP, D)
    outputs = lax.map(expert_apply, (per_expert, expert_gate, expert_up, expert_down))
    by_block = outputs.reshape(EXPERTS, block_count, CAP, D).transpose(1, 0, 2, 3).reshape(block_count, slot_count, D)
    chosen = jax.vmap(lambda block_out, slot_block: jnp.take(block_out, slot_block.reshape(-1), axis=0))(by_block, slots).reshape(-1, TOP_K, D)
    routed = lax.optimization_barrier(jnp.sum(route_weights[:, :, None] * chosen.astype(jnp.float32), axis=1))
    shared_hidden = swiglu_hidden(normed, shared_gate, shared_up)
    shared_sum = block_sum(shared_hidden, shared_down, SH_DEV)
    channel_out = (shared_sum + routed).astype(jnp.bfloat16)
    return (mixer_out, channel_out)
```

```python
import functools
import math

import jax
import jax.numpy as jnp
from jax import lax
from jax.experimental import pallas as pl
from jax.experimental.pallas import tpu as pltpu
from jax.sharding import PartitionSpec as P

GRID_W = 64


rope_base = 10000.0
norm_eps = 1e-06

MESH = pl.DeviceIdType.MESH


def greet(ep_count, tp_count, e, t):
    barrier = pltpu.get_barrier_semaphore()
    peers = 0
    for d in range(1, ep_count):
        pl.semaphore_signal(
            barrier, inc=1, device_id={"ep": lax.rem(e + d, ep_count)}, device_id_type=MESH
        )
        peers += 1
    pair = t // 2
    core = lax.rem(t, 2)
    for k in range(1, tp_count // 2):
        pl.semaphore_signal(
            barrier,
            inc=1,
            device_id={"tp": lax.rem(pair + k, tp_count // 2) * 2 + core},
            device_id_type=MESH,
        )
        peers += 1
    pl.semaphore_signal(
        barrier, inc=1, device_id={"tp": pair * 2 + 1 - core}, device_id_type=MESH
    )
    peers += 1
    return lambda: pl.semaphore_wait(barrier, peers)


def remote(src, dst, send, recv, device):
    return pltpu.make_async_remote_copy(
        src_ref=src,
        dst_ref=dst,
        send_sem=send,
        recv_sem=recv,
        device_id=device,
        device_id_type=MESH,
    )


def whole_kernel(
    ep_count,
    tp_count,
    direct,
    queries_hbm,
    kv_hbm,
    query_gain_hbm,
    key_gain_hbm,
    batch_hbm,
    norm_gain_hbm,
    routes_hbm,
    route_weights_hbm,
    out_weight_hbm,
    gate_hbm,
    up_hbm,
    down_hbm,
    shared_gate_hbm,
    shared_up_hbm,
    shared_down_hbm,
    channel_out,
    mixed_sum,
    queries,
    kv_in,
    head_gains,
    batch,
    norm_gain,
    routes,
    route_weights,
    tables,
    query,
    tokens,
    arrived,
    normed_all,
    kv_all,
    meta_ep,
    meta_tp,
    out_weight,
    gate,
    up,
    down,
    shared_both,
    shared_down,
    heads_scr,
    routed,
    shared,
    mixed,
    combined,
    returned,
    routed_pair,
    routed_out,
    routed_in,
    routed_done,
    shared_pair,
    shared_out,
    shared_in,
    mixed_pair,
    mixed_out,
    mixed_in,
    local_sem,
    kv_send,
    kv_recv,
    meta_send,
    meta_recv,
    z_send,
    z_recv,
    x_send,
    x_recv,
    d_send,
    d_recv,
    back_d_send,
    back_d_recv,
    back_x_send,
    back_x_recv,
    back_z_send,
    back_z_recv,
):
    e = lax.axis_index("ep")
    t = lax.axis_index("tp")
    half = tp_count // 2
    pair = t // 2
    core = lax.rem(t, 2)
    sibling = {"tp": pair * 2 + 1 - core}
    f32 = jnp.float32
    bf16 = jnp.bfloat16
    head_size = query_gain_hbm.shape[1]
    shared_width = shared_down.shape[0]
    loads = [
        pltpu.make_async_copy(source, target, local_sem.at[n])
        for n, (source, target) in enumerate(
            (
                (batch_hbm, batch),
                (norm_gain_hbm, norm_gain),
                (routes_hbm, routes),
                (route_weights_hbm, route_weights),
                (kv_hbm, kv_in),
                (query_gain_hbm, head_gains.at[0]),
                (key_gain_hbm, head_gains.at[1]),
                (queries_hbm, queries),
                (shared_gate_hbm, shared_both.at[:, :shared_width]),
                (shared_up_hbm, shared_both.at[:, shared_width:]),
                (gate_hbm, gate),
                (up_hbm, up),
                (down_hbm, down),
                (shared_down_hbm, shared_down),
                (out_weight_hbm, out_weight),
            )
        )
    ]
    for copy in loads:
        copy.start()
    greeted = greet(ep_count, tp_count, e, t)

    sends = []

    def send(src, dst, send_sem, recv_sem, device):
        copy = remote(src, dst, send_sem, recv_sem, device)
        copy.start()
        sends.append((None, copy.wait_send))

    def send_if(wanted, make):
        @pl.when(wanted)
        def _():
            make().start()

        sends.append((wanted, lambda: make().wait_send()))

    def landed(spot, recv_sem):
        remote(spot, spot, kv_send.at[0], recv_sem, sibling).wait_recv()

    near_side = jnp.minimum(e, ep_count - 1 - e)
    far_way = jnp.where(e < ep_count - 1 - e, 1, -1)

    def source_of(d):
        if d == 0:
            return e
        way = -1 if d % 2 else 1
        return jnp.where(
            d <= 2 * near_side, e + way * ((d + 1) // 2), e + far_way * (d - near_side)
        )

    tok_count, model_width = batch.shape
    local_count, capacity = arrived.shape[0], arrived.shape[3]
    near_count = local_count * capacity
    tile = min(512, model_width)

    def tiles(step):
        def run(m, ignored):
            step(pl.ds(pl.multiple_of(m * tile, tile), tile))
            return ignored

        lax.fori_loop(0, model_width // tile, run, 0)

    def picks_of(meta, rank, ranks=1):
        rows = ranks * near_count
        numbers = lax.broadcasted_iota(jnp.int32, (rows, tok_count), 0)
        expert = (numbers // capacity + rank * local_count).astype(f32)
        place = lax.rem(numbers, capacity).astype(f32)
        earlier = lax.broadcasted_iota(jnp.int32, (tok_count, tok_count), 0)
        later = lax.broadcasted_iota(jnp.int32, (tok_count, tok_count), 1)
        before = jnp.where(earlier < later, 1.0, 0.0).astype(bf16)
        named = [meta[j : j + 1, :] == expert for j in range(2)]
        any_named = sum(jnp.where(match, 1.0, 0.0) for match in named)
        count = jnp.dot(any_named.astype(bf16), before, preferred_element_type=f32)
        picked = jnp.where(count == place, any_named, 0.0)
        weight = sum(jnp.where(match, meta[2 + j : 3 + j, :], 0.0) for j, match in enumerate(named))
        return picked, picked * weight

    def split(value):
        high = value.astype(bf16)
        return high, (value - high.astype(f32)).astype(bf16)

    def place(d, row):
        if d == ep_count:
            return normed_all.at[row]
        if d == ep_count + 1:
            return meta_tp.at[row]
        return arrived.at[:, row, source_of(d)]

    def spread(src, d):
        for k in range(1, half):
            other = lax.rem(pair + k, half)
            send(
                src,
                place(d, t),
                x_send.at[k, d],
                x_recv.at[pair, d],
                {"tp": other * 2 + core},
            )
        send(src, place(d, t), d_send.at[0, d], d_recv.at[pair, d], sibling)

    def pass_on(d):
        for k in range(1, half):
            other = lax.rem(pair + k, half)
            spot = place(d, other * 2 + core)
            landed(spot, x_recv.at[other, d])
            send(spot, spot, d_send.at[k, d], d_recv.at[other, d], sibling)

    def all_here(d):
        for other in range(half):
            landed(place(d, other * 2 + 1 - core), d_recv.at[other, d])

    loads[0].wait()
    loads[1].wait()
    norm_rows = math.gcd(tok_count, 16)

    def norm_step(n, ignored):
        rows = pl.ds(pl.multiple_of(n * norm_rows, norm_rows), norm_rows)
        value = batch[rows, :].astype(f32)
        scale = lax.rsqrt(jnp.mean(value * value, axis=-1, keepdims=True) + norm_eps)
        normed_all[t, rows, :] = (value * scale * norm_gain[...]).astype(bf16)
        return ignored

    lax.fori_loop(0, tok_count // norm_rows, norm_step, 0)
    loads[2].wait()
    loads[3].wait()
    meta_tp[t, 0:2, :] = routes[...].astype(f32)
    meta_tp[t, 2:4, :] = route_weights[...]
    greeted()
    spread(normed_all.at[t], ep_count)
    if not direct:
        send_if(
            e < ep_count - 1,
            lambda: remote(
                normed_all.at[t], tokens.at[e], z_send.at[e], z_recv.at[e], {"ep": e + 1}
            ),
        )
        send_if(
            e > 0,
            lambda: remote(
                normed_all.at[t], tokens.at[e], z_send.at[ep_count], z_recv.at[e], {"ep": e - 1}
            ),
        )
    spread(meta_tp.at[t], ep_count + 1)
    if direct:
        picked, ignored_weight = picks_of(meta_tp[t], 0, ep_count)
        picked = picked.astype(bf16)

        def block_step(columns):
            part = jnp.dot(picked, normed_all[t, :, columns], preferred_element_type=f32)
            tokens[:, :, :, columns] = part.reshape(
                ep_count, local_count, capacity, tile
            ).astype(bf16)

        tiles(block_step)
        for d in range(1, ep_count):
            there = lax.rem(e + d, ep_count)
            send(
                tokens.at[there], arrived.at[:, t, e], z_send.at[d], z_recv.at[e], {"ep": there}
            )
    else:
        for d in range(1, ep_count):
            there = lax.rem(e + d, ep_count)
            send(meta_tp.at[t], meta_ep.at[e], meta_send.at[d], meta_recv.at[e], {"ep": there})

    query_rows, wide = query.shape[1], query.shape[2]
    groups = query_rows // GRID_W
    lane = lax.broadcasted_iota(jnp.int32, (GRID_W, wide), 1)
    low = lane < head_size

    def turn_tables():
        in_head = lax.rem(lane, head_size)
        step = lax.rem(in_head // 2, head_size // 4).astype(f32)
        inverse = jnp.exp(step * (-4.0 / head_size * math.log(rope_base)))
        number = lax.broadcasted_iota(jnp.int32, (GRID_W, wide), 0)
        sign = jnp.where(lax.rem(lane, 2) == 0, -1.0, 1.0)
        column_angle = number.astype(f32) * inverse
        tables[0] = jnp.cos(column_angle)
        tables[1] = jnp.sin(column_angle) * sign
        short = tables.shape[1] // 4
        row_angle = (number + e * groups).astype(f32)[:short] * inverse[:short]
        tables[2, :short] = jnp.cos(row_angle)
        tables[3, :short] = jnp.sin(row_angle) * sign[:short]

    def turn(value, group):
        by_row = lax.rem(lane, head_size) < head_size // 2
        cosine = jnp.where(by_row, tables[2, pl.ds(group, 1), :], tables[0])
        sine = jnp.where(by_row, tables[3, pl.ds(group, 1), :], tables[1])
        swapped = jnp.where(
            lax.rem(lane, 2) == 0, pltpu.roll(value, wide - 1, 1), pltpu.roll(value, 1, 1)
        )
        return value * cosine + swapped * sine

    def gain_of(n):
        value = head_gains[n]
        return jnp.concatenate([value] * (wide // head_size), axis=1)

    for n in (4, 5, 6):
        loads[n].wait()
    turn_tables()

    def key_step(group, ignored):
        rows = pl.ds(pl.multiple_of(group * GRID_W, GRID_W), GRID_W)
        value = kv_in[rows, :].astype(f32)
        square = jnp.sum(jnp.where(low, value * value, 0.0), axis=-1, keepdims=True)
        scaled = value * lax.rsqrt(square / head_size + norm_eps) * gain_of(1)
        kv_all[e, rows, :] = jnp.where(low, turn(scaled, group), value).astype(bf16)
        return ignored

    lax.fori_loop(0, groups, key_step, 0)
    for d in range(1, ep_count):
        there = lax.rem(e + d, ep_count)
        send(kv_all.at[e], kv_all.at[e], kv_send.at[d], kv_recv.at[e], {"ep": there})
    loads[7].wait()

    def query_step(group, ignored):
        rows = pl.ds(pl.multiple_of(group * GRID_W, GRID_W), GRID_W)
        for n in range(query.shape[0] // 2):
            value = queries[rows, n * wide : (n + 1) * wide].astype(f32)
            square = value * value
            sums = [
                jnp.sum(jnp.where(side, square, 0.0), axis=-1, keepdims=True)
                for side in (low, jnp.logical_not(low))
            ]
            scales = [lax.rsqrt(total / head_size + norm_eps) for total in sums]
            scaled = value * jnp.where(low, scales[0], scales[1]) * gain_of(0)
            turned = turn(scaled, group) * head_size ** (-0.5)
            query[2 * n, rows, :] = jnp.where(low, turned, 0.0).astype(bf16)
            query[2 * n + 1, rows, :] = jnp.where(
                low, pltpu.roll(turned, wide // 2, 1), 0.0
            ).astype(bf16)
        return ignored

    lax.fori_loop(0, groups, query_step, 0)

    def come(d):
        source = source_of(d)
        spot = arrived.at[:, t, source]
        if direct:
            landed(spot, z_recv.at[source])
        else:
            landed(tokens.at[source], z_recv.at[source])
            above = source > e
            send_if(
                jnp.logical_or(
                    jnp.logical_and(above, e > 0),
                    jnp.logical_and(jnp.logical_not(above), e < ep_count - 1),
                ),
                lambda: remote(
                    tokens.at[source],
                    tokens.at[source],
                    z_send.at[source],
                    z_recv.at[source],
                    {"ep": jnp.where(source > e, e - 1, e + 1)},
                ),
            )
            landed(meta_ep.at[source], meta_recv.at[source])
            picked, ignored_weight = picks_of(meta_ep[source], e)
            picked = picked.astype(bf16)

            def pick_step(columns):
                part = jnp.dot(picked, tokens[source, :, columns], preferred_element_type=f32)
                arrived[:, t, source, :, columns] = part.reshape(
                    local_count, capacity, tile
                ).astype(bf16)

            tiles(pick_step)
        spread(spot, d)

    def attend(h):
        def step(b, carried):
            top_now, total_now, acc_now = carried
            block = kv_all[b]
            scores = lax.dot_general(
                query[h], block, (((1,), (1,)), ((), ())), preferred_element_type=f32
            )
            top_new = jnp.maximum(top_now, jnp.max(scores, axis=-1, keepdims=True))
            shrink = jnp.exp(top_now - top_new)
            exps = jnp.exp(scores - top_new)
            total_new = total_now * shrink + jnp.sum(exps, axis=-1, keepdims=True)
            acc_new = acc_now * shrink + jnp.dot(
                exps.astype(bf16), block, preferred_element_type=f32
            )
            return (top_new, total_new, acc_new)

        start = (
            jnp.full((query_rows, 1), -1e30, f32),
            jnp.zeros((query_rows, 1), f32),
            jnp.zeros((query_rows, wide), f32),
        )
        top, total, acc = lax.fori_loop(0, ep_count, step, start)
        return acc / total

    def attend_two(n):
        low = pltpu.roll(attend(2 * n), wide // 2, 1)
        high = attend(2 * n + 1)
        lane = lax.broadcasted_iota(jnp.int32, low.shape, 1)
        heads_scr[:, n * wide : (n + 1) * wide] = jnp.where(lane < wide // 2, low, high).astype(
            bf16
        )

    def project():
        def step(n, ignored):
            columns = pl.ds(pl.multiple_of(n * tile, tile), tile)
            part = jnp.dot(heads_scr[...], out_weight[:, columns], preferred_element_type=f32)
            mixed[:, :, columns] = part.astype(bf16).reshape(
                tp_count, query_rows // tp_count, tile
            )
            return ignored

        lax.fori_loop(0, model_width // tile, step, 0)

    def share():
        def step(row, ignored):
            both_parts = jnp.dot(normed_all[row], shared_both[...], preferred_element_type=f32)
            gate_part = both_parts[:, :shared_width]
            up_part = both_parts[:, shared_width:]
            hidden = (gate_part / (1.0 + jnp.exp(-gate_part)) * up_part).astype(bf16)
            ignored_pick, weight = picks_of(meta_tp[row], e)
            weights = split(weight)

            def columns_step(columns):
                results = routed[:, row, e, :, columns]
                if capacity % 16:
                    results = results.astype(f32)
                results = results.reshape(near_count, tile).astype(bf16)
                part = jnp.dot(hidden, shared_down[:, columns], preferred_element_type=f32)
                for one in weights:
                    part = part + lax.dot_general(
                        one, results, (((0,), (0,)), ((), ())), preferred_element_type=f32
                    )
                shared[row, :, columns] = part.astype(bf16)

            tiles(columns_step)
            return ignored

        lax.fori_loop(0, tp_count, step, 0)

    def pick_own():
        def step(row, ignored):
            picked, ignored_weight = picks_of(meta_tp[row], e)
            picked = picked.astype(bf16)

            def columns_step(columns):
                part = jnp.dot(picked, normed_all[row, :, columns], preferred_element_type=f32)
                arrived[:, row, e, :, columns] = part.reshape(
                    local_count, capacity, tile
                ).astype(bf16)

            tiles(columns_step)
            return ignored

        lax.fori_loop(0, tp_count, step, 0)

    def experts(d):
        source = source_of(d)

        def step(n, ignored):
            rows = arrived[n, :, source]
            if capacity % 16:
                rows = rows.astype(f32)
            rows = rows.reshape(tp_count * capacity, model_width).astype(bf16)
            gate_part = jnp.dot(rows, gate[n], preferred_element_type=f32)
            up_part = jnp.dot(rows, up[n], preferred_element_type=f32)
            hidden = (gate_part / (1.0 + jnp.exp(-gate_part)) * up_part).astype(bf16)

            def columns_step(m, inner):
                columns = pl.ds(pl.multiple_of(m * tile, tile), tile)
                part = jnp.dot(hidden, down[n, :, columns], preferred_element_type=f32)
                if capacity % 16:
                    part = part.reshape(tp_count, capacity, tile).astype(bf16)
                else:
                    part = part.astype(bf16).reshape(tp_count, capacity, tile)
                routed[n, :, source, :, columns] = part
                return inner

            lax.fori_loop(0, model_width // tile, columns_step, 0)
            return ignored

        lax.fori_loop(0, local_count, step, 0)

    def item(d):
        if d < ep_count:
            source = source_of(d)
            return (
                lambda row: routed.at[:, row, source],
                lambda k: routed_pair.at[d, k],
                lambda k: routed_out.at[d, k - 1],
                lambda k: routed_in.at[d, k - 1],
            )
        if d == ep_count:
            return (
                lambda row: shared.at[row],
                lambda k: shared_pair.at[k],
                lambda k: shared_out.at[k - 1],
                lambda k: shared_in.at[k - 1],
            )
        return (
            lambda row: mixed.at[row],
            lambda k: mixed_pair.at[k],
            lambda k: mixed_out.at[k - 1],
            lambda k: mixed_in.at[k - 1],
        )

    def to_sibling(d):
        part, paired, out, into = item(d)
        for k in list(range(1, half)) + [0]:
            other = lax.rem(pair + k, half)
            send(
                part(other * 2 + 1 - core),
                paired(k),
                back_d_send.at[d, k],
                back_d_recv.at[d, k],
                sibling,
            )

    def both(d, k):
        part, paired, out, into = item(d)
        spot = paired(k)
        landed(spot, back_d_recv.at[d, k])
        mine = part(lax.rem(pair + k, half) * 2 + core)
        return mine[...].astype(f32) + spot[...].astype(f32)

    def across(d):
        part, paired, out, into = item(d)
        for k in range(1, half):
            other = lax.rem(pair + k, half)
            out(k)[...] = both(d, k).astype(bf16)
            send(
                out(k),
                into(k),
                back_x_send.at[d, k],
                back_x_recv.at[d, k],
                {"tp": other * 2 + core},
            )

    def finish(d):
        part, paired, out, into = item(d)
        total = both(d, 0)
        for k in range(1, half):
            spot = into(k)
            landed(spot, back_x_recv.at[d, k])
            total = total + spot[...].astype(f32)
        if d < ep_count:
            routed_done[d] = total.astype(bf16)
            send(
                routed_done.at[d],
                returned.at[e],
                back_z_send.at[d],
                back_z_recv.at[e],
                {"ep": source_of(d)},
            )
        elif d == ep_count:
            channel_out[...] = (total + combined[...]).astype(bf16)
        else:
            mixed_sum[...] = total.astype(bf16)

    def combine(d):
        source = source_of(d)
        landed(returned.at[source], back_z_recv.at[source])
        ignored_pick, weight = picks_of(meta_tp[t], source)
        weights = split(weight)

        def columns_step(columns):
            results = returned[source, :, :, columns]
            if capacity % 16:
                results = results.astype(f32)
            results = results.reshape(near_count, tile).astype(bf16)
            part = sum(
                lax.dot_general(
                    one, results, (((0,), (0,)), ((), ())), preferred_element_type=f32
                )
                for one in weights
            )
            combined[:, columns] = part if d == 1 else combined[:, columns] + part

        tiles(columns_step)

    last = ep_count - 1
    pair_count = query.shape[0] // 2

    def expert_item(d):
        all_here(d)
        experts(d)
        to_sibling(d)

    def attention():
        for d in range(1, ep_count):
            landed(kv_all.at[source_of(d)], kv_recv.at[source_of(d)])
        for n in range(pair_count):
            attend_two(n)
        loads[14].wait()
        project()
        to_sibling(ep_count + 1)

    pass_on(ep_count + 1)
    pass_on(ep_count)
    come(1)
    all_here(ep_count + 1)
    all_here(ep_count)
    pick_own()
    for n in range(8, 14):
        loads[n].wait()
    experts(0)
    share()
    to_sibling(ep_count)
    for d in range(2, ep_count):
        come(d)
        pass_on(d - 1)
        expert_item(d - 1)
        across(d - 1)
        if d == 2:
            attention()
        if d > 2:
            finish(d - 2)
    pass_on(last)
    expert_item(last)
    across(last)
    across(ep_count + 1)
    across(ep_count)
    for d in range(max(1, last - 1), ep_count):
        finish(d)
    finish(ep_count + 1)
    for d in range(1, ep_count):
        combine(d)
    finish(ep_count)
    for wanted, wait in sends:
        if wanted is None:
            wait()
        else:
            pl.when(wanted)(wait)


def whole(ep_count, tp_count, small, weights):
    queries, key_values, query_gain, key_gain, batch, norm_gain, routes, route_weights = small
    out_weight, gate, up, down, shared_gate, shared_up, shared_down = weights
    local_count = gate.shape[0]
    tok_count, width = batch.shape
    query_rows, wide = key_values.shape
    head_size = query_gain.shape[1]
    heads_here = queries.shape[1] // head_size
    expert_count = local_count * ep_count
    capacity = 3 * tok_count * routes.shape[0] // (2 * expert_count)
    capacity = (capacity + 7) // 8 * 8
    direct = 2 * local_count * capacity <= tok_count
    anywhere = pl.BlockSpec(memory_space=pl.ANY)
    half = tp_count // 2
    dma = pltpu.SemaphoreType.DMA
    block = (local_count, capacity, width)
    spread_block = (local_count, tp_count, ep_count, capacity, width)
    token_block = (tok_count, width)
    mixed = (query_rows // tp_count, width)
    count = ep_count + 2

    def room(*shape):
        return pltpu.VMEM(shape, jnp.bfloat16)

    def wide_room(*shape):
        return pltpu.VMEM(shape, jnp.float32)

    return pl.pallas_call(
        functools.partial(whole_kernel, ep_count, tp_count, direct),
        out_shape=(
            jax.ShapeDtypeStruct(token_block, jnp.bfloat16),
            jax.ShapeDtypeStruct(mixed, jnp.bfloat16),
        ),
        in_specs=[anywhere] * (len(small) + len(weights)),
        out_specs=(pl.BlockSpec(memory_space=pltpu.VMEM),) * 2,
        scratch_shapes=[
            room(*queries.shape),
            room(*key_values.shape),
            wide_room(2, 1, head_size),
            room(*batch.shape),
            wide_room(*norm_gain.shape),
            pltpu.VMEM(routes.shape, jnp.int32),
            wide_room(*route_weights.shape),
            wide_room(4, GRID_W, wide),
            room(heads_here, query_rows, wide),
            room(*((ep_count,) + (block if direct else token_block))),
            room(*spread_block),
            room(tp_count, *token_block),
            room(ep_count, *key_values.shape),
            wide_room(ep_count, 8, tok_count),
            wide_room(tp_count, 8, tok_count),
            room(*out_weight.shape),
            room(*gate.shape),
            room(*up.shape),
            room(*down.shape),
            room(shared_gate.shape[0], 2 * shared_gate.shape[1]),
            room(*shared_down.shape),
            room(query_rows, heads_here // 2 * wide),
            room(*spread_block),
            room(tp_count, *token_block),
            room(tp_count, *mixed),
            wide_room(*token_block),
            room(ep_count, *block),
            room(ep_count, half, *block),
            room(ep_count, half - 1, *block),
            room(ep_count, half - 1, *block),
            room(ep_count, *block),
            room(half, *token_block),
            room(half - 1, *token_block),
            room(half - 1, *token_block),
            room(half, *mixed),
            room(half - 1, *mixed),
            room(half - 1, *mixed),
            dma((len(small) + len(weights),)),
            dma((ep_count,)),
            dma((ep_count,)),
            dma((ep_count,)),
            dma((ep_count,)),
            dma((ep_count + 1,)),
            dma((ep_count,)),
            dma((half, ep_count + 2)),
            dma((half, ep_count + 2)),
            dma((half, ep_count + 2)),
            dma((half, ep_count + 2)),
            dma((count, half)),
            dma((count, half)),
            dma((count, half)),
            dma((count, half)),
            dma((ep_count,)),
            dma((ep_count,)),
        ],
        compiler_params=pltpu.CompilerParams(
            collective_id=0, has_side_effects=True, vmem_limit_bytes=67043328
        ),
    )(*small, *weights)


def body(
    queries,
    key_values,
    query_gain,
    key_gain,
    out_weight,
    second_batch,
    norm_gain,
    routes,
    route_weights,
    expert_gate,
    expert_up,
    expert_down,
    shared_gate,
    shared_up,
    shared_down,
):
    channel_out, mixer_out = whole(
        lax.axis_size("ep"),
        lax.axis_size("tp"),
        (
            queries,
            key_values,
            query_gain[None, :],
            key_gain[None, :],
            second_batch,
            norm_gain[None, :],
            routes.T,
            route_weights.T,
        ),
        (
            out_weight,
            expert_gate,
            expert_up,
            expert_down,
            shared_gate,
            shared_up,
            shared_down,
        ),
    )
    return (mixer_out, channel_out)


def solution(mesh):
    placed = (
        P(("grp", "ep"), "tp"),
        P(("grp", "ep"), "tp"),
        P(),
        P(),
        P("tp", None),
        P(("grp", "ep", "tp"), None),
        P(),
        P(("grp", "ep", "tp"), None),
        P(("grp", "ep", "tp"), None),
        P("ep", None, "tp"),
        P("ep", None, "tp"),
        P("ep", "tp", None),
        P(None, "tp"),
        P(None, "tp"),
        P("tp", None),
    )
    return jax.shard_map(
        body,
        mesh=mesh,
        in_specs=placed,
        out_specs=(P(("grp", "ep", "tp"), None), P(("grp", "ep", "tp"), None)),
        check_vma=False,
    )
```

```python
import functools
import math

import jax
import jax.numpy as jnp
from jax import lax
from jax.experimental import pallas as pl
from jax.experimental.pallas import tpu as pltpu
from jax.sharding import PartitionSpec as P

GRID_W = 64


rope_base = 10000.0
norm_eps = 1e-06

MESH = pl.DeviceIdType.MESH


def greet(ep_count, tp_count, e, t):
    barrier = pltpu.get_barrier_semaphore()
    peers = 0
    for d in range(1, ep_count):
        pl.semaphore_signal(
            barrier, inc=1, device_id={"ep": lax.rem(e + d, ep_count)}, device_id_type=MESH
        )
        peers += 1
    pair = t // 2
    core = lax.rem(t, 2)
    for k in range(1, tp_count // 2):
        pl.semaphore_signal(
            barrier,
            inc=1,
            device_id={"tp": lax.rem(pair + k, tp_count // 2) * 2 + core},
            device_id_type=MESH,
        )
        peers += 1
    pl.semaphore_signal(
        barrier, inc=1, device_id={"tp": pair * 2 + 1 - core}, device_id_type=MESH
    )
    peers += 1
    return lambda: pl.semaphore_wait(barrier, peers)


def remote(src, dst, send, recv, device):
    return pltpu.make_async_remote_copy(
        src_ref=src,
        dst_ref=dst,
        send_sem=send,
        recv_sem=recv,
        device_id=device,
        device_id_type=MESH,
    )


def whole_kernel(
    ep_count,
    tp_count,
    direct,
    queries_hbm,
    kv_hbm,
    query_gain_hbm,
    key_gain_hbm,
    batch_hbm,
    norm_gain_hbm,
    routes_hbm,
    route_weights_hbm,
    out_weight_hbm,
    gate_hbm,
    up_hbm,
    down_hbm,
    shared_gate_hbm,
    shared_up_hbm,
    shared_down_hbm,
    channel_out,
    mixed_sum,
    queries,
    kv_in,
    head_gains,
    batch,
    norm_gain,
    routes,
    route_weights,
    tables,
    query,
    tokens,
    arrived,
    normed_all,
    kv_all,
    meta_ep,
    meta_tp,
    out_weight,
    gate,
    up,
    down,
    shared_both,
    shared_down,
    heads_scr,
    routed,
    shared,
    mixed,
    hidden,
    weights_here,
    combined,
    returned,
    onward,
    lent_out,
    lent_in,
    routed_pair,
    routed_out,
    routed_in,
    routed_done,
    shared_pair,
    shared_out,
    shared_in,
    mixed_pair,
    mixed_out,
    mixed_in,
    local_sem,
    kv_send,
    kv_recv,
    meta_send,
    meta_recv,
    lent_send,
    lent_recv,
    r_send,
    r_recv,
    z_send,
    z_recv,
    x_send,
    x_recv,
    d_send,
    d_recv,
    back_d_send,
    back_d_recv,
    back_x_send,
    back_x_recv,
    back_z_send,
    back_z_recv,
):
    e = lax.axis_index("ep")
    t = lax.axis_index("tp")
    half = tp_count // 2
    pair = t // 2
    core = lax.rem(t, 2)
    sibling = {"tp": pair * 2 + 1 - core}
    f32 = jnp.float32
    bf16 = jnp.bfloat16
    head_size = query_gain_hbm.shape[1]
    shared_width = shared_down.shape[0]
    loads = [
        pltpu.make_async_copy(source, target, local_sem.at[n])
        for n, (source, target) in enumerate(
            (
                (batch_hbm, batch),
                (norm_gain_hbm, norm_gain),
                (routes_hbm, routes),
                (route_weights_hbm, route_weights),
                (kv_hbm, kv_in),
                (query_gain_hbm, head_gains.at[0]),
                (key_gain_hbm, head_gains.at[1]),
                (queries_hbm, queries),
                (shared_gate_hbm, shared_both.at[:, :shared_width]),
                (shared_up_hbm, shared_both.at[:, shared_width:]),
                (gate_hbm, gate),
                (up_hbm, up),
                (down_hbm, down),
                (shared_down_hbm, shared_down),
                (out_weight_hbm, out_weight),
            )
        )
    ]
    for copy in loads:
        copy.start()
    greeted = greet(ep_count, tp_count, e, t)

    sends = []

    state = {"start": True, "note": True, "when": None}

    def send(src, dst, send_sem, recv_sem, device):
        copy = remote(src, dst, send_sem, recv_sem, device)
        if state["start"]:
            copy.start()
        if state["note"]:
            sends.append((state["when"], copy.wait_send))

    def branch(when, *steps):
        @pl.when(when)
        def _():
            state["note"] = False
            for step in steps:
                step()
            state["note"] = True

    def note(when, *steps):
        state.update(start=False, when=when)
        for step in steps:
            step()
        state.update(start=True, when=None)

    def send_if(wanted, make):
        @pl.when(wanted)
        def _():
            make().start()

        sends.append((wanted, lambda: make().wait_send()))

    def landed(spot, recv_sem):
        if state["start"]:
            remote(spot, spot, kv_send.at[0], recv_sem, sibling).wait_recv()

    near_side = jnp.minimum(e, ep_count - 1 - e)
    far_way = jnp.where(e < ep_count - 1 - e, 1, -1)

    def source_of(d):
        if d == 0:
            return e
        way = far_way if d % 2 else -far_way
        return jnp.where(
            d <= 2 * near_side, e + way * ((d + 1) // 2), e + far_way * (d - near_side)
        )

    def first_of(rank):
        inner = jnp.where(rank < ep_count - 1 - rank, rank - 1, rank + 1)
        return jnp.where(rank == 0, 1, jnp.where(rank == ep_count - 1, ep_count - 2, inner))

    tok_count, model_width = batch.shape
    local_count, capacity = arrived.shape[0], arrived.shape[3]
    near_count = local_count * capacity
    tile = min(512, model_width)

    def tiles(step, first=0, stop=model_width):
        def run(m, ignored):
            step(pl.ds(pl.multiple_of(m * tile, tile), tile))
            return ignored

        lax.fori_loop(first // tile, stop // tile, run, 0)

    half_width = model_width // 2
    sides = [(c * half_width, (c + 1) * half_width) for c in range(2)]

    def picks_of(meta, rank, ranks=1):
        rows = ranks * near_count
        numbers = lax.broadcasted_iota(jnp.int32, (rows, tok_count), 0)
        expert = (numbers // capacity + rank * local_count).astype(f32)
        place = lax.rem(numbers, capacity).astype(f32)
        earlier = lax.broadcasted_iota(jnp.int32, (tok_count, tok_count), 0)
        later = lax.broadcasted_iota(jnp.int32, (tok_count, tok_count), 1)
        before = jnp.where(earlier < later, 1.0, 0.0).astype(bf16)
        named = [meta[j : j + 1, :] == expert for j in range(2)]
        any_named = sum(jnp.where(match, 1.0, 0.0) for match in named)
        count = jnp.dot(any_named.astype(bf16), before, preferred_element_type=f32)
        picked = jnp.where(count == place, any_named, 0.0)
        weight = sum(jnp.where(match, meta[2 + j : 3 + j, :], 0.0) for j, match in enumerate(named))
        return picked, picked * weight

    def split(value):
        high = value.astype(bf16)
        return high, (value - high.astype(f32)).astype(bf16)

    def place(d, row):
        if d == ep_count:
            return normed_all.at[row]
        if d == ep_count + 1:
            return meta_tp.at[row]
        return arrived.at[:, row, source_of(d)]

    def spread(src, d):
        for k in range(1, half):
            other = lax.rem(pair + k, half)
            send(
                src,
                place(d, t),
                x_send.at[k, d],
                x_recv.at[pair, d],
                {"tp": other * 2 + core},
            )
        send(src, place(d, t), d_send.at[0, d], d_recv.at[pair, d], sibling)

    def pass_on(d):
        for k in range(1, half):
            other = lax.rem(pair + k, half)
            spot = place(d, other * 2 + core)
            landed(spot, x_recv.at[other, d])
            send(spot, spot, d_send.at[k, d], d_recv.at[other, d], sibling)

    def all_here(d, kinds=range(half)):
        for k in kinds:
            other = lax.rem(pair + k, half)
            landed(place(d, other * 2 + 1 - core), d_recv.at[other, d])

    loads[0].wait()
    loads[1].wait()
    norm_rows = math.gcd(tok_count, 16)

    def norm_step(n, ignored):
        rows = pl.ds(pl.multiple_of(n * norm_rows, norm_rows), norm_rows)
        value = batch[rows, :].astype(f32)
        scale = lax.rsqrt(jnp.mean(value * value, axis=-1, keepdims=True) + norm_eps)
        normed_all[t, rows, :] = (value * scale * norm_gain[...]).astype(bf16)
        return ignored

    lax.fori_loop(0, tok_count // norm_rows, norm_step, 0)
    loads[2].wait()
    loads[3].wait()
    meta_tp[t, 0:2, :] = routes[...].astype(f32)
    meta_tp[t, 2:4, :] = route_weights[...]
    greeted()
    spread(normed_all.at[t], ep_count)
    if not direct:
        send_if(
            e < ep_count - 1,
            lambda: remote(
                normed_all.at[t], tokens.at[e], z_send.at[e], z_recv.at[e], {"ep": e + 1}
            ),
        )
        send_if(
            e > 0,
            lambda: remote(
                normed_all.at[t], tokens.at[e], z_send.at[ep_count], z_recv.at[e], {"ep": e - 1}
            ),
        )
    spread(meta_tp.at[t], ep_count + 1)
    if direct:
        picked, ignored_weight = picks_of(meta_tp[t], 0, ep_count)
        picked = picked.astype(bf16)

        def block_step(columns):
            part = jnp.dot(picked, normed_all[t, :, columns], preferred_element_type=f32)
            tokens[:, :, :, columns] = part.reshape(
                ep_count, local_count, capacity, tile
            ).astype(bf16)

        tiles(block_step)
        for d in range(1, ep_count):
            there = lax.rem(e + d, ep_count)
            send(
                tokens.at[there], arrived.at[:, t, e], z_send.at[d], z_recv.at[e], {"ep": there}
            )
    else:
        for d in range(1, ep_count):
            there = lax.rem(e + d, ep_count)
            send(meta_tp.at[t], meta_ep.at[e], meta_send.at[d], meta_recv.at[e], {"ep": there})

    query_rows, wide = query.shape[1], query.shape[2]
    groups = query_rows // GRID_W
    lane = lax.broadcasted_iota(jnp.int32, (GRID_W, wide), 1)
    low = lane < head_size

    def turn_tables():
        in_head = lax.rem(lane, head_size)
        step = lax.rem(in_head // 2, head_size // 4).astype(f32)
        inverse = jnp.exp(step * (-4.0 / head_size * math.log(rope_base)))
        number = lax.broadcasted_iota(jnp.int32, (GRID_W, wide), 0)
        sign = jnp.where(lax.rem(lane, 2) == 0, -1.0, 1.0)
        column_angle = number.astype(f32) * inverse
        tables[0] = jnp.cos(column_angle)
        tables[1] = jnp.sin(column_angle) * sign
        short = tables.shape[1] // 4
        row_angle = (number + e * groups).astype(f32)[:short] * inverse[:short]
        tables[2, :short] = jnp.cos(row_angle)
        tables[3, :short] = jnp.sin(row_angle) * sign[:short]

    def turn(value, group):
        by_row = lax.rem(lane, head_size) < head_size // 2
        cosine = jnp.where(by_row, tables[2, pl.ds(group, 1), :], tables[0])
        sine = jnp.where(by_row, tables[3, pl.ds(group, 1), :], tables[1])
        swapped = jnp.where(
            lax.rem(lane, 2) == 0, pltpu.roll(value, wide - 1, 1), pltpu.roll(value, 1, 1)
        )
        return value * cosine + swapped * sine

    def gain_of(n):
        value = head_gains[n]
        return jnp.concatenate([value] * (wide // head_size), axis=1)

    for n in (4, 5, 6):
        loads[n].wait()
    turn_tables()

    def key_step(group, ignored):
        rows = pl.ds(pl.multiple_of(group * GRID_W, GRID_W), GRID_W)
        value = kv_in[rows, :].astype(f32)
        square = jnp.sum(jnp.where(low, value * value, 0.0), axis=-1, keepdims=True)
        scaled = value * lax.rsqrt(square / head_size + norm_eps) * gain_of(1)
        kv_all[e, rows, :] = jnp.where(low, turn(scaled, group), value).astype(bf16)
        return ignored

    lax.fori_loop(0, groups, key_step, 0)
    loads[7].wait()

    def query_step(group, ignored):
        rows = pl.ds(pl.multiple_of(group * GRID_W, GRID_W), GRID_W)
        for n in range(query.shape[0] // 2):
            value = queries[rows, n * wide : (n + 1) * wide].astype(f32)
            square = value * value
            sums = [
                jnp.sum(jnp.where(side, square, 0.0), axis=-1, keepdims=True)
                for side in (low, jnp.logical_not(low))
            ]
            scales = [lax.rsqrt(total / head_size + norm_eps) for total in sums]
            scaled = value * jnp.where(low, scales[0], scales[1]) * gain_of(0)
            turned = turn(scaled, group) * head_size ** (-0.5)
            query[2 * n, rows, :] = jnp.where(low, turned, 0.0).astype(bf16)
            query[2 * n + 1, rows, :] = jnp.where(
                low, pltpu.roll(turned, wide // 2, 1), 0.0
            ).astype(bf16)
        return ignored

    lax.fori_loop(0, groups, query_step, 0)

    early = near_side > 0
    late = jnp.logical_not(early)

    def pick_into(source, rank, target, first=0, stop=model_width):
        picked, ignored_weight = picks_of(meta_ep[source], rank)
        picked = picked.astype(bf16)

        def pick_step(columns):
            part = jnp.dot(picked, tokens[source, :, columns], preferred_element_type=f32)
            target(columns, part.reshape(local_count, capacity, tile).astype(bf16))

        tiles(pick_step, first, stop)

    def relay(d, parts=(0, 1)):
        if direct:
            return
        source = source_of(d)
        target = jnp.where(source > e, e - 1, e + 1)
        to_end = jnp.logical_or(target == 0, target == ep_count - 1)
        whole_rows = jnp.logical_and(early, jnp.logical_not(to_end))
        picked_rows = jnp.logical_and(early, to_end)

        @pl.when(early)
        def _():
            if d <= 2:
                landed(tokens.at[source], z_recv.at[source])
            if 0 in parts:
                landed(meta_ep.at[source], meta_recv.at[source])

        for c in parts:
            first, stop = sides[c]
            if d > 2:

                @pl.when(early)
                def _():
                    landed(tokens.at[source, :, first:stop], r_recv.at[source, c])

            def rows_copy(c=c, first=first, stop=stop):
                spot = tokens.at[source, :, first:stop]
                return remote(
                    spot, spot, r_send.at[source, c], r_recv.at[source, c], {"ep": target}
                )

            def slots_copy(c=c, first=first, stop=stop):
                return remote(
                    onward.at[d - 1, :, :, first:stop],
                    arrived.at[:, t, source, :, first:stop],
                    r_send.at[source, c],
                    r_recv.at[source, c],
                    {"ep": target},
                )

            send_if(whole_rows, rows_copy)

            @pl.when(picked_rows)
            def _():
                def put(columns, value):
                    onward[d - 1, :, :, columns] = value

                pick_into(source, target, put, first, stop)

            send_if(picked_rows, slots_copy)

    def pick_here(d):
        source = source_of(d)

        def put(columns, value):
            arrived[:, t, source, :, columns] = value

        pick_into(source, e, put)

    def come(d):
        source = source_of(d)
        spot = arrived.at[:, t, source]
        if direct:
            landed(spot, z_recv.at[source])
        elif d == 1:

            @pl.when(late)
            def _():
                landed(tokens.at[source], z_recv.at[source])
                landed(meta_ep.at[source], meta_recv.at[source])

            pick_here(d)
        else:

            @pl.when(late)
            def _():
                for c, (first, stop) in enumerate(sides):
                    landed(spot.at[:, :, first:stop], r_recv.at[source, c])
                landed(meta_ep.at[source], meta_recv.at[source])

            @pl.when(early)
            def _():
                pick_here(d)

        spread(spot, d)

    def send_keys():
        for d in range(1, ep_count):
            there = lax.rem(e + d, ep_count)
            send(kv_all.at[e], kv_all.at[e], kv_send.at[d], kv_recv.at[e], {"ep": there})

    def attend(h):
        def step(b, carried):
            top_now, total_now, acc_now = carried
            block = kv_all[b]
            scores = lax.dot_general(
                query[h], block, (((1,), (1,)), ((), ())), preferred_element_type=f32
            )
            top_new = jnp.maximum(top_now, jnp.max(scores, axis=-1, keepdims=True))
            shrink = jnp.exp(top_now - top_new)
            exps = jnp.exp(scores - top_new)
            total_new = total_now * shrink + jnp.sum(exps, axis=-1, keepdims=True)
            acc_new = acc_now * shrink + jnp.dot(
                exps.astype(bf16), block, preferred_element_type=f32
            )
            return (top_new, total_new, acc_new)

        start = (
            jnp.full((query_rows, 1), -1e30, f32),
            jnp.zeros((query_rows, 1), f32),
            jnp.zeros((query_rows, wide), f32),
        )
        top, total, acc = lax.fori_loop(0, ep_count, step, start)
        return acc / total

    def attend_two(n):
        low = pltpu.roll(attend(2 * n), wide // 2, 1)
        high = attend(2 * n + 1)
        lane = lax.broadcasted_iota(jnp.int32, low.shape, 1)
        heads_scr[:, n * wide : (n + 1) * wide] = jnp.where(lane < wide // 2, low, high).astype(
            bf16
        )

    def project():
        def step(n, ignored):
            columns = pl.ds(pl.multiple_of(n * tile, tile), tile)
            part = jnp.dot(heads_scr[...], out_weight[:, columns], preferred_element_type=f32)
            mixed[:, :, columns] = part.astype(bf16).reshape(
                tp_count, query_rows // tp_count, tile
            )
            return ignored

        lax.fori_loop(0, model_width // tile, step, 0)

    def begin(row):
        both_parts = jnp.dot(normed_all[row], shared_both[...], preferred_element_type=f32)
        gate_part = both_parts[:, :shared_width]
        up_part = both_parts[:, shared_width:]
        hidden[row] = (gate_part / (1.0 + jnp.exp(-gate_part)) * up_part).astype(bf16)
        picked, weight = picks_of(meta_tp[row], e)
        for n, part in enumerate(split(weight)):
            weights_here[row, n] = part
        picked = picked.astype(bf16)

        def columns_step(columns):
            part = jnp.dot(picked, normed_all[row, :, columns], preferred_element_type=f32)
            arrived[:, row, e, :, columns] = part.reshape(local_count, capacity, tile).astype(
                bf16
            )

        tiles(columns_step)

    def begin_pair(which):
        def step(n, ignored):
            begin(which * 2 + n)
            return ignored

        lax.fori_loop(0, 2, step, 0)

    def share():
        def step(row, ignored):
            def columns_step(columns):
                results = routed[:, row, e, :, columns]
                if capacity % 16:
                    results = results.astype(f32)
                results = results.reshape(near_count, tile).astype(bf16)
                part = jnp.dot(
                    hidden[row], shared_down[:, columns], preferred_element_type=f32
                )
                for n in range(2):
                    part = part + lax.dot_general(
                        weights_here[row, n],
                        results,
                        (((0,), (0,)), ((), ())),
                        preferred_element_type=f32,
                    )
                shared[row, :, columns] = part.astype(bf16)

            tiles(columns_step)
            return ignored

        lax.fori_loop(0, tp_count, step, 0)

    def experts(d):
        source = source_of(d)

        def step(n, ignored):
            rows = arrived[n, :, source]
            if capacity % 16:
                rows = rows.astype(f32)
            rows = rows.reshape(tp_count * capacity, model_width).astype(bf16)
            gate_part = jnp.dot(rows, gate[n], preferred_element_type=f32)
            up_part = jnp.dot(rows, up[n], preferred_element_type=f32)
            hidden = (gate_part / (1.0 + jnp.exp(-gate_part)) * up_part).astype(bf16)

            def columns_step(m, inner):
                columns = pl.ds(pl.multiple_of(m * tile, tile), tile)
                part = jnp.dot(hidden, down[n, :, columns], preferred_element_type=f32)
                if capacity % 16:
                    part = part.reshape(tp_count, capacity, tile).astype(bf16)
                else:
                    part = part.astype(bf16).reshape(tp_count, capacity, tile)
                routed[n, :, source, :, columns] = part
                return inner

            lax.fori_loop(0, model_width // tile, columns_step, 0)
            return ignored

        lax.fori_loop(0, local_count, step, 0)

    def item(d):
        if d < ep_count:
            source = source_of(d)
            return (
                lambda row: routed.at[:, row, source],
                lambda k: routed_pair.at[d, k],
                lambda k: routed_out.at[d, k - 1],
                lambda k: routed_in.at[d, k - 1],
            )
        if d == ep_count:
            return (
                lambda row: shared.at[row],
                lambda k: shared_pair.at[k],
                lambda k: shared_out.at[k - 1],
                lambda k: shared_in.at[k - 1],
            )
        return (
            lambda row: mixed.at[row],
            lambda k: mixed_pair.at[k],
            lambda k: mixed_out.at[k - 1],
            lambda k: mixed_in.at[k - 1],
        )

    def to_sibling(d):
        part, paired, out, into = item(d)
        for k in list(range(1, half)) + [0]:
            other = lax.rem(pair + k, half)
            send(
                part(other * 2 + 1 - core),
                paired(k),
                back_d_send.at[d, k],
                back_d_recv.at[d, k],
                sibling,
            )

    def both(d, k):
        part, paired, out, into = item(d)
        spot = paired(k)
        landed(spot, back_d_recv.at[d, k])
        mine = part(lax.rem(pair + k, half) * 2 + core)
        return mine[...].astype(f32) + spot[...].astype(f32)

    def across(d):
        part, paired, out, into = item(d)
        for k in range(1, half):
            other = lax.rem(pair + k, half)
            if state["start"]:
                out(k)[...] = both(d, k).astype(bf16)
            send(
                out(k),
                into(k),
                back_x_send.at[d, k],
                back_x_recv.at[d, k],
                {"tp": other * 2 + core},
            )

    def finish(d):
        part, paired, out, into = item(d)
        if state["start"]:
            total = both(d, 0)
            for k in range(1, half):
                spot = into(k)
                landed(spot, back_x_recv.at[d, k])
                total = total + spot[...].astype(f32)
            if d > ep_count:
                mixed_sum[...] = total.astype(bf16)
                return
            routed_done[d] = total.astype(bf16)
        send(
            routed_done.at[d],
            returned.at[e],
            back_z_send.at[d],
            back_z_recv.at[e],
            {"ep": source_of(d)},
        )

    def lend(d):
        home = source_of(d)
        side = jnp.where(home > e, 0, 1)
        for k in range(half):
            if state["start"]:
                lent_out[k] = both(d, k).astype(bf16)
            send(
                lent_out.at[k],
                lent_in.at[side, k],
                lent_send.at[k],
                lent_recv.at[side, k],
                {"ep": home},
            )

    def add_results(results_of, meta, rank, target=None):
        ignored_pick, weight = picks_of(meta, rank)
        weights = split(weight)

        def columns_step(columns):
            results = results_of(columns)
            if capacity % 16:
                results = results.astype(f32)
            results = results.reshape(near_count, tile).astype(bf16)
            part = sum(
                lax.dot_general(
                    one, results, (((0,), (0,)), ((), ())), preferred_element_type=f32
                )
                for one in weights
            )
            total = combined[:, columns] + part
            if target is None:
                combined[:, columns] = total
            else:
                target[:, columns] = total.astype(bf16)

        tiles(columns_step)

    def gather(k):
        combined[...] = both(ep_count, k)
        row = lax.rem(pair + k, half) * 2 + core
        below = jnp.logical_and(e > 0, first_of(e - 1) == e)
        above = jnp.logical_and(e < ep_count - 1, first_of(e + 1) == e)
        for side, there, rank in ((0, below, e - 1), (1, above, e + 1)):

            @pl.when(there)
            def _():
                landed(lent_in.at[side, k], lent_recv.at[side, k])
                add_results(
                    lambda columns: lent_in[side, k, :, :, columns], meta_tp[row], rank
                )

    def share_across():
        part, paired, out, into = item(ep_count)
        for k in range(1, half):
            gather(k)
            out(k)[...] = combined[...].astype(bf16)
            send(
                out(k),
                into(k),
                back_x_send.at[ep_count, k],
                back_x_recv.at[ep_count, k],
                {"tp": lax.rem(pair + k, half) * 2 + core},
            )
        gather(0)

    def share_finish():
        part, paired, out, into = item(ep_count)
        for k in range(1, half):
            landed(into(k), back_x_recv.at[ep_count, k])
            combined[...] = combined[...] + into(k)[...].astype(f32)

    def combine(d):
        source = source_of(d)
        landed(returned.at[source], back_z_recv.at[source])
        add_results(
            lambda columns: returned[source, :, :, columns],
            meta_tp[t],
            source,
            channel_out if d == ep_count - 1 else None,
        )

    last = ep_count - 1
    pair_count = query.shape[0] // 2

    def expert_item(d):
        all_here(d)
        experts(d)
        to_sibling(d)

    for n in range(8, 14):
        loads[n].wait()
    all_here(ep_count + 1, (0,))
    all_here(ep_count, (0,))
    begin_pair(pair)
    pass_on(ep_count + 1)
    pass_on(ep_count)
    relay(2)
    relay(1)
    come(1)
    branch(early, lambda: come(2))
    for k in range(1, half):
        all_here(ep_count + 1, (k,))
        all_here(ep_count, (k,))
        begin_pair(lax.rem(pair + k, half))
    experts(0)
    relay(3, (0,))
    pass_on(1)
    relay(3, (1,))
    branch(late, lambda: come(2))
    note(None, lambda: spread(arrived.at[:, t, source_of(2)], 2))
    expert_item(1)
    send_keys()
    branch(late, lambda: lend(1))
    branch(early, lambda: across(1))
    come(3)
    pass_on(2)
    expert_item(2)

    def out_part():
        for n in range(1, pair_count):
            attend_two(n)
        loads[14].wait()
        project()
        to_sibling(ep_count + 1)

    def third():
        pass_on(3)
        expert_item(3)
        across(3)

    branch(late, lambda: across(2))
    branch(early, lambda: lend(2))
    for d in range(1, ep_count):
        landed(kv_all.at[source_of(d)], kv_recv.at[source_of(d)])
    attend_two(0)
    branch(early, lambda: finish(1), out_part, lambda: across(ep_count + 1), third)
    branch(late, third, lambda: finish(2), out_part, lambda: across(ep_count + 1))
    note(
        None,
        lambda: pass_on(3),
        lambda: to_sibling(3),
        lambda: across(3),
        lambda: to_sibling(ep_count + 1),
        lambda: across(ep_count + 1),
    )
    note(late, lambda: lend(1), lambda: across(2), lambda: finish(2))
    note(early, lambda: lend(2), lambda: across(1), lambda: finish(1))
    for d in range(4, ep_count):
        relay(d)
        come(d)
        pass_on(d)
        expert_item(d)
        across(d)
    share()
    to_sibling(ep_count)
    for d in range(3, ep_count):
        finish(d)
    share_across()
    finish(ep_count + 1)
    share_finish()
    for d in (1, 2):
        pl.when(first_of(source_of(d)) != e)(functools.partial(combine, d))
    for d in range(3, ep_count):
        combine(d)
    for wanted, wait in sends:
        if wanted is None:
            wait()
        else:
            pl.when(wanted)(wait)


def whole(ep_count, tp_count, small, weights):
    queries, key_values, query_gain, key_gain, batch, norm_gain, routes, route_weights = small
    out_weight, gate, up, down, shared_gate, shared_up, shared_down = weights
    local_count = gate.shape[0]
    tok_count, width = batch.shape
    query_rows, wide = key_values.shape
    head_size = query_gain.shape[1]
    heads_here = queries.shape[1] // head_size
    expert_count = local_count * ep_count
    capacity = 3 * tok_count * routes.shape[0] // (2 * expert_count)
    capacity = (capacity + 7) // 8 * 8
    direct = 2 * local_count * capacity <= tok_count
    anywhere = pl.BlockSpec(memory_space=pl.ANY)
    half = tp_count // 2
    dma = pltpu.SemaphoreType.DMA
    block = (local_count, capacity, width)
    spread_block = (local_count, tp_count, ep_count, capacity, width)
    token_block = (tok_count, width)
    mixed = (query_rows // tp_count, width)
    count = ep_count + 2

    def room(*shape):
        return pltpu.VMEM(shape, jnp.bfloat16)

    def wide_room(*shape):
        return pltpu.VMEM(shape, jnp.float32)

    return pl.pallas_call(
        functools.partial(whole_kernel, ep_count, tp_count, direct),
        out_shape=(
            jax.ShapeDtypeStruct(token_block, jnp.bfloat16),
            jax.ShapeDtypeStruct(mixed, jnp.bfloat16),
        ),
        in_specs=[anywhere] * (len(small) + len(weights)),
        out_specs=(pl.BlockSpec(memory_space=pltpu.VMEM),) * 2,
        scratch_shapes=[
            room(*queries.shape),
            room(*key_values.shape),
            wide_room(2, 1, head_size),
            room(*batch.shape),
            wide_room(*norm_gain.shape),
            pltpu.VMEM(routes.shape, jnp.int32),
            wide_room(*route_weights.shape),
            wide_room(4, GRID_W, wide),
            room(heads_here, query_rows, wide),
            room(*((ep_count,) + (block if direct else token_block))),
            room(*spread_block),
            room(tp_count, *token_block),
            room(ep_count, *key_values.shape),
            wide_room(ep_count, 8, tok_count),
            wide_room(tp_count, 8, tok_count),
            room(*out_weight.shape),
            room(*gate.shape),
            room(*up.shape),
            room(*down.shape),
            room(shared_gate.shape[0], 2 * shared_gate.shape[1]),
            room(*shared_down.shape),
            room(query_rows, heads_here // 2 * wide),
            room(*spread_block),
            room(tp_count, *token_block),
            room(tp_count, *mixed),
            room(tp_count, tok_count, shared_down.shape[0]),
            room(tp_count, 2, local_count * capacity, tok_count),
            wide_room(*token_block),
            room(ep_count, *block),
            room(*((1 if direct else ep_count - 1,) + block)),
            room(half, *block),
            room(2, half, *block),
            room(ep_count, half, *block),
            room(ep_count, half - 1, *block),
            room(ep_count, half - 1, *block),
            room(ep_count, *block),
            room(half, *token_block),
            room(half - 1, *token_block),
            room(half - 1, *token_block),
            room(half, *mixed),
            room(half - 1, *mixed),
            room(half - 1, *mixed),
            dma((len(small) + len(weights),)),
            dma((ep_count,)),
            dma((ep_count,)),
            dma((ep_count,)),
            dma((ep_count,)),
            dma((half,)),
            dma((2, half)),
            dma((ep_count, 2)),
            dma((ep_count, 2)),
            dma((ep_count + 1,)),
            dma((ep_count,)),
            dma((half, ep_count + 2)),
            dma((half, ep_count + 2)),
            dma((half, ep_count + 2)),
            dma((half, ep_count + 2)),
            dma((count, half)),
            dma((count, half)),
            dma((count, half)),
            dma((count, half)),
            dma((ep_count,)),
            dma((ep_count,)),
        ],
        compiler_params=pltpu.CompilerParams(
            collective_id=0, has_side_effects=True, vmem_limit_bytes=67043328
        ),
    )(*small, *weights)


def settle_kernel(*refs):
    count = (len(refs) - 1) // 3
    sources, targets, rooms = (refs[n * count : (n + 1) * count] for n in range(3))
    sem = refs[-1]
    moves = []
    for n, (source, room, target) in enumerate(zip(sources, rooms, targets)):
        rows = source.shape[0] // 2
        for c in range(2):
            part = pl.ds(c * rows, rows)
            taken = pltpu.make_async_copy(source.at[part], room.at[part], sem.at[0, n, c])
            given = pltpu.make_async_copy(room.at[part], target.at[part], sem.at[1, n, c])
            taken.start()
            moves.append((taken, given))
    for taken, given in moves:
        taken.wait()
        given.start()
    for taken, given in moves:
        given.wait()


def settle(*arrays):
    anywhere = pl.BlockSpec(memory_space=pl.ANY)
    return pl.pallas_call(
        settle_kernel,
        out_shape=tuple(jax.ShapeDtypeStruct(a.shape, a.dtype) for a in arrays),
        in_specs=[anywhere] * len(arrays),
        out_specs=(anywhere,) * len(arrays),
        scratch_shapes=[pltpu.VMEM(a.shape, a.dtype) for a in arrays]
        + [pltpu.SemaphoreType.DMA((2, len(arrays), 2))],
    )(*arrays)


def body(
    queries,
    key_values,
    query_gain,
    key_gain,
    out_weight,
    second_batch,
    norm_gain,
    routes,
    route_weights,
    expert_gate,
    expert_up,
    expert_down,
    shared_gate,
    shared_up,
    shared_down,
):
    channel_out, mixer_out = whole(
        lax.axis_size("ep"),
        lax.axis_size("tp"),
        (
            queries,
            key_values,
            query_gain[None, :],
            key_gain[None, :],
            second_batch,
            norm_gain[None, :],
            routes.T,
            route_weights.T,
        ),
        (
            out_weight,
            expert_gate,
            expert_up,
            expert_down,
            shared_gate,
            shared_up,
            shared_down,
        ),
    )
    return settle(mixer_out, channel_out)


def solution(mesh):
    placed = (
        P(("grp", "ep"), "tp"),
        P(("grp", "ep"), "tp"),
        P(),
        P(),
        P("tp", None),
        P(("grp", "ep", "tp"), None),
        P(),
        P(("grp", "ep", "tp"), None),
        P(("grp", "ep", "tp"), None),
        P("ep", None, "tp"),
        P("ep", None, "tp"),
        P("ep", "tp", None),
        P(None, "tp"),
        P(None, "tp"),
        P("tp", None),
    )
    return jax.shard_map(
        body,
        mesh=mesh,
        in_specs=placed,
        out_specs=(P(("grp", "ep", "tp"), None), P(("grp", "ep", "tp"), None)),
        check_vma=False,
    )
```

```python
import functools
import math

import jax
import jax.numpy as jnp
from jax import lax
from jax.experimental import pallas as pl
from jax.experimental.pallas import tpu as pltpu
from jax.sharding import PartitionSpec as P

GRID_W = 64


rope_base = 10000.0
norm_eps = 1e-06

MESH = pl.DeviceIdType.MESH


def greet(ep_count, tp_count, e, t):
    barrier = pltpu.get_barrier_semaphore()
    peers = 0
    for d in range(1, ep_count):
        pl.semaphore_signal(
            barrier, inc=1, device_id={"ep": lax.rem(e + d, ep_count)}, device_id_type=MESH
        )
        peers += 1
    pair = t // 2
    core = lax.rem(t, 2)
    for k in range(1, tp_count // 2):
        pl.semaphore_signal(
            barrier,
            inc=1,
            device_id={"tp": lax.rem(pair + k, tp_count // 2) * 2 + core},
            device_id_type=MESH,
        )
        peers += 1
    pl.semaphore_signal(
        barrier, inc=1, device_id={"tp": pair * 2 + 1 - core}, device_id_type=MESH
    )
    peers += 1
    return lambda: pl.semaphore_wait(barrier, peers)


def remote(src, dst, send, recv, device):
    return pltpu.make_async_remote_copy(
        src_ref=src,
        dst_ref=dst,
        send_sem=send,
        recv_sem=recv,
        device_id=device,
        device_id_type=MESH,
    )


def whole_kernel(
    ep_count,
    tp_count,
    direct,
    queries_hbm,
    kv_hbm,
    query_gain_hbm,
    key_gain_hbm,
    batch_hbm,
    norm_gain_hbm,
    routes_hbm,
    route_weights_hbm,
    out_weight_hbm,
    gate_hbm,
    up_hbm,
    down_hbm,
    shared_gate_hbm,
    shared_up_hbm,
    shared_down_hbm,
    channel_out,
    mixed_sum,
    queries,
    kv_in,
    head_gains,
    batch,
    norm_gain,
    routes,
    route_weights,
    tables,
    query,
    tokens,
    arrived,
    normed_all,
    kv_all,
    meta_ep,
    meta_tp,
    out_weight,
    gate,
    up,
    down,
    shared_both,
    shared_down,
    heads_scr,
    routed,
    shared,
    mixed,
    hidden,
    weights_here,
    combined,
    returned,
    onward,
    lent_out,
    lent_in,
    routed_pair,
    routed_out,
    routed_in,
    routed_done,
    shared_pair,
    shared_out,
    shared_in,
    mixed_pair,
    mixed_out,
    mixed_in,
    local_sem,
    kv_send,
    kv_recv,
    meta_send,
    meta_recv,
    lent_send,
    lent_recv,
    r_send,
    r_recv,
    z_send,
    z_recv,
    x_send,
    x_recv,
    d_send,
    d_recv,
    back_d_send,
    back_d_recv,
    back_x_send,
    back_x_recv,
    back_z_send,
    back_z_recv,
):
    e = lax.axis_index("ep")
    t = lax.axis_index("tp")
    half = tp_count // 2
    pair = t // 2
    core = lax.rem(t, 2)
    sibling = {"tp": pair * 2 + 1 - core}
    f32 = jnp.float32
    bf16 = jnp.bfloat16
    head_size = query_gain_hbm.shape[1]
    shared_width = shared_down.shape[0]
    loads = [
        pltpu.make_async_copy(source, target, local_sem.at[n])
        for n, (source, target) in enumerate(
            (
                (batch_hbm, batch),
                (norm_gain_hbm, norm_gain),
                (routes_hbm, routes),
                (route_weights_hbm, route_weights),
                (kv_hbm, kv_in),
                (query_gain_hbm, head_gains.at[0]),
                (key_gain_hbm, head_gains.at[1]),
                (queries_hbm, queries),
                (shared_gate_hbm, shared_both.at[:, :shared_width]),
                (shared_up_hbm, shared_both.at[:, shared_width:]),
                (gate_hbm, gate),
                (up_hbm, up),
                (down_hbm, down),
                (shared_down_hbm, shared_down),
                (out_weight_hbm, out_weight),
            )
        )
    ]
    for copy in loads:
        copy.start()
    greeted = greet(ep_count, tp_count, e, t)

    sends = []

    state = {"start": True, "note": True, "when": None}

    def send(src, dst, send_sem, recv_sem, device):
        copy = remote(src, dst, send_sem, recv_sem, device)
        if state["start"]:
            copy.start()
        if state["note"]:
            sends.append((state["when"], copy.wait_send))

    def branch(when, *steps):
        @pl.when(when)
        def _():
            state["note"] = False
            for step in steps:
                step()
            state["note"] = True

    def note(when, *steps):
        state.update(start=False, when=when)
        for step in steps:
            step()
        state.update(start=True, when=None)

    def send_if(wanted, make):
        @pl.when(wanted)
        def _():
            make().start()

        sends.append((wanted, lambda: make().wait_send()))

    def landed(spot, recv_sem):
        if state["start"]:
            remote(spot, spot, kv_send.at[0], recv_sem, sibling).wait_recv()

    near_side = jnp.minimum(e, ep_count - 1 - e)
    far_way = jnp.where(e < ep_count - 1 - e, 1, -1)

    def source_of(d):
        if d == 0:
            return e
        way = far_way if d % 2 else -far_way
        return jnp.where(
            d <= 2 * near_side, e + way * ((d + 1) // 2), e + far_way * (d - near_side)
        )

    def first_of(rank):
        inner = jnp.where(rank < ep_count - 1 - rank, rank - 1, rank + 1)
        return jnp.where(rank == 0, 1, jnp.where(rank == ep_count - 1, ep_count - 2, inner))

    tok_count, model_width = batch.shape
    local_count, capacity = arrived.shape[0], arrived.shape[3]
    near_count = local_count * capacity
    tile = min(512, model_width)

    def tiles(step, first=0, stop=model_width):
        def run(m, ignored):
            step(pl.ds(pl.multiple_of(m * tile, tile), tile))
            return ignored

        lax.fori_loop(first // tile, stop // tile, run, 0)

    half_width = model_width // 2
    sides = [(c * half_width, (c + 1) * half_width) for c in range(2)]

    def picks_of(meta, rank, ranks=1):
        rows = ranks * near_count
        numbers = lax.broadcasted_iota(jnp.int32, (rows, tok_count), 0)
        expert = (numbers // capacity + rank * local_count).astype(f32)
        place = lax.rem(numbers, capacity).astype(f32)
        earlier = lax.broadcasted_iota(jnp.int32, (tok_count, tok_count), 0)
        later = lax.broadcasted_iota(jnp.int32, (tok_count, tok_count), 1)
        before = jnp.where(earlier < later, 1.0, 0.0).astype(bf16)
        named = [meta[j : j + 1, :] == expert for j in range(2)]
        any_named = sum(jnp.where(match, 1.0, 0.0) for match in named)
        count = jnp.dot(any_named.astype(bf16), before, preferred_element_type=f32)
        picked = jnp.where(count == place, any_named, 0.0)
        weight = sum(jnp.where(match, meta[2 + j : 3 + j, :], 0.0) for j, match in enumerate(named))
        return picked, picked * weight

    def split(value):
        high = value.astype(bf16)
        return high, (value - high.astype(f32)).astype(bf16)

    def place(d, row):
        if d == ep_count:
            return normed_all.at[row]
        if d == ep_count + 1:
            return meta_tp.at[row]
        return arrived.at[:, row, source_of(d)]

    def spread(src, d):
        for k in range(1, half):
            other = lax.rem(pair + k, half)
            send(
                src,
                place(d, t),
                x_send.at[k, d],
                x_recv.at[pair, d],
                {"tp": other * 2 + core},
            )
        send(src, place(d, t), d_send.at[0, d], d_recv.at[pair, d], sibling)

    def pass_on(d):
        for k in range(1, half):
            other = lax.rem(pair + k, half)
            spot = place(d, other * 2 + core)
            landed(spot, x_recv.at[other, d])
            send(spot, spot, d_send.at[k, d], d_recv.at[other, d], sibling)

    def all_here(d, kinds=range(half)):
        for k in kinds:
            other = lax.rem(pair + k, half)
            landed(place(d, other * 2 + 1 - core), d_recv.at[other, d])

    loads[0].wait()
    loads[1].wait()
    norm_rows = math.gcd(tok_count, 16)

    def norm_step(n, ignored):
        rows = pl.ds(pl.multiple_of(n * norm_rows, norm_rows), norm_rows)
        value = batch[rows, :].astype(f32)
        scale = lax.rsqrt(jnp.mean(value * value, axis=-1, keepdims=True) + norm_eps)
        normed_all[t, rows, :] = (value * scale * norm_gain[...]).astype(bf16)
        return ignored

    lax.fori_loop(0, tok_count // norm_rows, norm_step, 0)
    loads[2].wait()
    loads[3].wait()
    meta_tp[t, 0:2, :] = routes[...].astype(f32)
    meta_tp[t, 2:4, :] = route_weights[...]
    greeted()
    spread(normed_all.at[t], ep_count)
    if not direct:
        send_if(
            e < ep_count - 1,
            lambda: remote(
                normed_all.at[t], tokens.at[e], z_send.at[e], z_recv.at[e], {"ep": e + 1}
            ),
        )
        send_if(
            e > 0,
            lambda: remote(
                normed_all.at[t], tokens.at[e], z_send.at[ep_count], z_recv.at[e], {"ep": e - 1}
            ),
        )
    spread(meta_tp.at[t], ep_count + 1)
    if direct:
        picked, ignored_weight = picks_of(meta_tp[t], 0, ep_count)
        picked = picked.astype(bf16)

        def block_step(columns):
            part = jnp.dot(picked, normed_all[t, :, columns], preferred_element_type=f32)
            tokens[:, :, :, columns] = part.reshape(
                ep_count, local_count, capacity, tile
            ).astype(bf16)

        tiles(block_step)
        for d in range(1, ep_count):
            there = lax.rem(e + d, ep_count)
            send(
                tokens.at[there], arrived.at[:, t, e], z_send.at[d], z_recv.at[e], {"ep": there}
            )
    else:
        for d in range(1, ep_count):
            there = lax.rem(e + d, ep_count)
            send(meta_tp.at[t], meta_ep.at[e], meta_send.at[d], meta_recv.at[e], {"ep": there})

    query_rows, wide = query.shape[1], query.shape[2]
    groups = query_rows // GRID_W
    lane = lax.broadcasted_iota(jnp.int32, (GRID_W, wide), 1)
    low = lane < head_size

    def turn_tables():
        in_head = lax.rem(lane, head_size)
        step = lax.rem(in_head // 2, head_size // 4).astype(f32)
        inverse = jnp.exp(step * (-4.0 / head_size * math.log(rope_base)))
        number = lax.broadcasted_iota(jnp.int32, (GRID_W, wide), 0)
        sign = jnp.where(lax.rem(lane, 2) == 0, -1.0, 1.0)
        column_angle = number.astype(f32) * inverse
        tables[0] = jnp.cos(column_angle)
        tables[1] = jnp.sin(column_angle) * sign
        short = tables.shape[1] // 4
        row_angle = (number + e * groups).astype(f32)[:short] * inverse[:short]
        tables[2, :short] = jnp.cos(row_angle)
        tables[3, :short] = jnp.sin(row_angle) * sign[:short]

    def turn(value, group):
        by_row = lax.rem(lane, head_size) < head_size // 2
        cosine = jnp.where(by_row, tables[2, pl.ds(group, 1), :], tables[0])
        sine = jnp.where(by_row, tables[3, pl.ds(group, 1), :], tables[1])
        swapped = jnp.where(
            lax.rem(lane, 2) == 0, pltpu.roll(value, wide - 1, 1), pltpu.roll(value, 1, 1)
        )
        return value * cosine + swapped * sine

    def gain_of(n):
        value = head_gains[n]
        return jnp.concatenate([value] * (wide // head_size), axis=1)

    for n in (4, 5, 6):
        loads[n].wait()
    turn_tables()

    def key_step(group, ignored):
        rows = pl.ds(pl.multiple_of(group * GRID_W, GRID_W), GRID_W)
        value = kv_in[rows, :].astype(f32)
        square = jnp.sum(jnp.where(low, value * value, 0.0), axis=-1, keepdims=True)
        scaled = value * lax.rsqrt(square / head_size + norm_eps) * gain_of(1)
        kv_all[e, rows, :] = jnp.where(low, turn(scaled, group), value).astype(bf16)
        return ignored

    lax.fori_loop(0, groups, key_step, 0)
    loads[7].wait()

    def query_step(group, ignored):
        rows = pl.ds(pl.multiple_of(group * GRID_W, GRID_W), GRID_W)
        for n in range(query.shape[0] // 2):
            value = queries[rows, n * wide : (n + 1) * wide].astype(f32)
            square = value * value
            sums = [
                jnp.sum(jnp.where(side, square, 0.0), axis=-1, keepdims=True)
                for side in (low, jnp.logical_not(low))
            ]
            scales = [lax.rsqrt(total / head_size + norm_eps) for total in sums]
            scaled = value * jnp.where(low, scales[0], scales[1]) * gain_of(0)
            turned = turn(scaled, group) * head_size ** (-0.5)
            query[2 * n, rows, :] = jnp.where(low, turned, 0.0).astype(bf16)
            query[2 * n + 1, rows, :] = jnp.where(
                low, pltpu.roll(turned, wide // 2, 1), 0.0
            ).astype(bf16)
        return ignored

    lax.fori_loop(0, groups, query_step, 0)

    early = near_side > 0
    late = jnp.logical_not(early)

    def pick_into(source, rank, target, first=0, stop=model_width):
        picked, ignored_weight = picks_of(meta_ep[source], rank)
        picked = picked.astype(bf16)

        def pick_step(columns):
            part = jnp.dot(picked, tokens[source, :, columns], preferred_element_type=f32)
            target(columns, part.reshape(local_count, capacity, tile).astype(bf16))

        tiles(pick_step, first, stop)

    def relay(d, parts=(0, 1)):
        if direct:
            return
        source = source_of(d)
        target = jnp.where(source > e, e - 1, e + 1)
        to_end = jnp.logical_or(target == 0, target == ep_count - 1)
        whole_rows = jnp.logical_and(early, jnp.logical_not(to_end))
        picked_rows = jnp.logical_and(early, to_end)

        @pl.when(early)
        def _():
            if d <= 2:
                landed(tokens.at[source], z_recv.at[source])
            if 0 in parts:
                landed(meta_ep.at[source], meta_recv.at[source])

        for c in parts:
            first, stop = sides[c]
            if d > 2:

                @pl.when(early)
                def _():
                    landed(tokens.at[source, :, first:stop], r_recv.at[source, c])

            def rows_copy(c=c, first=first, stop=stop):
                spot = tokens.at[source, :, first:stop]
                return remote(
                    spot, spot, r_send.at[source, c], r_recv.at[source, c], {"ep": target}
                )

            def slots_copy(c=c, first=first, stop=stop):
                return remote(
                    onward.at[d - 1, :, :, first:stop],
                    arrived.at[:, t, source, :, first:stop],
                    r_send.at[source, c],
                    r_recv.at[source, c],
                    {"ep": target},
                )

            send_if(whole_rows, rows_copy)

            @pl.when(picked_rows)
            def _():
                def put(columns, value):
                    onward[d - 1, :, :, columns] = value

                pick_into(source, target, put, first, stop)

            send_if(picked_rows, slots_copy)

    def pick_here(d):
        source = source_of(d)

        def put(columns, value):
            arrived[:, t, source, :, columns] = value

        pick_into(source, e, put)

    def come(d):
        source = source_of(d)
        spot = arrived.at[:, t, source]
        if direct:
            landed(spot, z_recv.at[source])
        elif d == 1:

            @pl.when(late)
            def _():
                landed(tokens.at[source], z_recv.at[source])
                landed(meta_ep.at[source], meta_recv.at[source])

            pick_here(d)
        else:

            @pl.when(late)
            def _():
                for c, (first, stop) in enumerate(sides):
                    landed(spot.at[:, :, first:stop], r_recv.at[source, c])
                landed(meta_ep.at[source], meta_recv.at[source])

            @pl.when(early)
            def _():
                pick_here(d)

        spread(spot, d)

    def send_keys():
        for d in range(1, ep_count):
            there = lax.rem(e + d, ep_count)
            send(kv_all.at[e], kv_all.at[e], kv_send.at[d], kv_recv.at[e], {"ep": there})

    def attend(h):
        def step(b, carried):
            top_now, total_now, acc_now = carried
            block = kv_all[b]
            scores = lax.dot_general(
                query[h], block, (((1,), (1,)), ((), ())), preferred_element_type=f32
            )
            top_new = jnp.maximum(top_now, jnp.max(scores, axis=-1, keepdims=True))
            shrink = jnp.exp(top_now - top_new)
            exps = jnp.exp(scores - top_new)
            total_new = total_now * shrink + jnp.sum(exps, axis=-1, keepdims=True)
            acc_new = acc_now * shrink + jnp.dot(
                exps.astype(bf16), block, preferred_element_type=f32
            )
            return (top_new, total_new, acc_new)

        start = (
            jnp.full((query_rows, 1), -1e30, f32),
            jnp.zeros((query_rows, 1), f32),
            jnp.zeros((query_rows, wide), f32),
        )
        top, total, acc = lax.fori_loop(0, ep_count, step, start)
        return acc / total

    def attend_two(n):
        low = pltpu.roll(attend(2 * n), wide // 2, 1)
        high = attend(2 * n + 1)
        lane = lax.broadcasted_iota(jnp.int32, low.shape, 1)
        heads_scr[:, n * wide : (n + 1) * wide] = jnp.where(lane < wide // 2, low, high).astype(
            bf16
        )

    def project():
        def step(n, ignored):
            columns = pl.ds(pl.multiple_of(n * tile, tile), tile)
            part = jnp.dot(heads_scr[...], out_weight[:, columns], preferred_element_type=f32)
            mixed[:, :, columns] = part.astype(bf16).reshape(
                tp_count, query_rows // tp_count, tile
            )
            return ignored

        lax.fori_loop(0, model_width // tile, step, 0)

    def begin(row):
        both_parts = jnp.dot(normed_all[row], shared_both[...], preferred_element_type=f32)
        gate_part = both_parts[:, :shared_width]
        up_part = both_parts[:, shared_width:]
        hidden[row] = (gate_part / (1.0 + jnp.exp(-gate_part)) * up_part).astype(bf16)
        picked, weight = picks_of(meta_tp[row], e)
        for n, part in enumerate(split(weight)):
            weights_here[row, n] = part
        picked = picked.astype(bf16)

        def columns_step(columns):
            part = jnp.dot(picked, normed_all[row, :, columns], preferred_element_type=f32)
            arrived[:, row, e, :, columns] = part.reshape(local_count, capacity, tile).astype(
                bf16
            )

        tiles(columns_step)

    def begin_pair(which):
        def step(n, ignored):
            begin(which * 2 + n)
            return ignored

        lax.fori_loop(0, 2, step, 0)

    def share():
        def step(row, ignored):
            def columns_step(columns):
                results = routed[:, row, e, :, columns]
                if capacity % 16:
                    results = results.astype(f32)
                results = results.reshape(near_count, tile).astype(bf16)
                part = jnp.dot(
                    hidden[row], shared_down[:, columns], preferred_element_type=f32
                )
                for n in range(2):
                    part = part + lax.dot_general(
                        weights_here[row, n],
                        results,
                        (((0,), (0,)), ((), ())),
                        preferred_element_type=f32,
                    )
                shared[row, :, columns] = part.astype(bf16)

            tiles(columns_step)
            return ignored

        lax.fori_loop(0, tp_count, step, 0)

    def experts(d):
        source = source_of(d)

        def step(n, ignored):
            rows = arrived[n, :, source]
            if capacity % 16:
                rows = rows.astype(f32)
            rows = rows.reshape(tp_count * capacity, model_width).astype(bf16)
            gate_part = jnp.dot(rows, gate[n], preferred_element_type=f32)
            up_part = jnp.dot(rows, up[n], preferred_element_type=f32)
            hidden = (gate_part / (1.0 + jnp.exp(-gate_part)) * up_part).astype(bf16)

            def columns_step(m, inner):
                columns = pl.ds(pl.multiple_of(m * tile, tile), tile)
                part = jnp.dot(hidden, down[n, :, columns], preferred_element_type=f32)
                if capacity % 16:
                    part = part.reshape(tp_count, capacity, tile).astype(bf16)
                else:
                    part = part.astype(bf16).reshape(tp_count, capacity, tile)
                routed[n, :, source, :, columns] = part
                return inner

            lax.fori_loop(0, model_width // tile, columns_step, 0)
            return ignored

        lax.fori_loop(0, local_count, step, 0)

    def item(d):
        if d < ep_count:
            source = source_of(d)
            return (
                lambda row: routed.at[:, row, source],
                lambda k: routed_pair.at[d, k],
                lambda k: routed_out.at[d, k - 1],
                lambda k: routed_in.at[d, k - 1],
            )
        if d == ep_count:
            return (
                lambda row: shared.at[row],
                lambda k: shared_pair.at[k],
                lambda k: shared_out.at[k - 1],
                lambda k: shared_in.at[k - 1],
            )
        return (
            lambda row: mixed.at[row],
            lambda k: mixed_pair.at[k],
            lambda k: mixed_out.at[k - 1],
            lambda k: mixed_in.at[k - 1],
        )

    def to_sibling(d):
        part, paired, out, into = item(d)
        for k in list(range(1, half)) + [0]:
            other = lax.rem(pair + k, half)
            send(
                part(other * 2 + 1 - core),
                paired(k),
                back_d_send.at[d, k],
                back_d_recv.at[d, k],
                sibling,
            )

    def both(d, k):
        part, paired, out, into = item(d)
        spot = paired(k)
        landed(spot, back_d_recv.at[d, k])
        mine = part(lax.rem(pair + k, half) * 2 + core)
        return mine[...].astype(f32) + spot[...].astype(f32)

    def across(d):
        part, paired, out, into = item(d)
        for k in range(1, half):
            other = lax.rem(pair + k, half)
            if state["start"]:
                out(k)[...] = both(d, k).astype(bf16)
            send(
                out(k),
                into(k),
                back_x_send.at[d, k],
                back_x_recv.at[d, k],
                {"tp": other * 2 + core},
            )

    def finish(d):
        part, paired, out, into = item(d)
        if state["start"]:
            total = both(d, 0)
            for k in range(1, half):
                spot = into(k)
                landed(spot, back_x_recv.at[d, k])
                total = total + spot[...].astype(f32)
            if d > ep_count:
                mixed_sum[...] = total.astype(bf16)
                return
            routed_done[d] = total.astype(bf16)
        send(
            routed_done.at[d],
            returned.at[e],
            back_z_send.at[d],
            back_z_recv.at[e],
            {"ep": source_of(d)},
        )

    def lend(d):
        home = source_of(d)
        side = jnp.where(home > e, 0, 1)
        for k in list(range(1, half)) + [0]:
            if state["start"]:
                lent_out[k] = both(d, k).astype(bf16)
            send(
                lent_out.at[k],
                lent_in.at[side, k],
                lent_send.at[k],
                lent_recv.at[side, k],
                {"ep": home},
            )

    def add_results(results_of, meta, rank):
        ignored_pick, weight = picks_of(meta, rank)
        weights = split(weight)

        def columns_step(columns):
            results = results_of(columns)
            if capacity % 16:
                results = results.astype(f32)
            results = results.reshape(near_count, tile).astype(bf16)
            part = sum(
                lax.dot_general(
                    one, results, (((0,), (0,)), ((), ())), preferred_element_type=f32
                )
                for one in weights
            )
            combined[:, columns] = combined[:, columns] + part

        tiles(columns_step)

    def gather(k):
        combined[...] = both(ep_count, k)
        row = lax.rem(pair + k, half) * 2 + core
        below = jnp.logical_and(e > 0, first_of(e - 1) == e)
        above = jnp.logical_and(e < ep_count - 1, first_of(e + 1) == e)
        for side, there, rank in ((0, below, e - 1), (1, above, e + 1)):

            @pl.when(there)
            def _():
                landed(lent_in.at[side, k], lent_recv.at[side, k])
                add_results(
                    lambda columns: lent_in[side, k, :, :, columns], meta_tp[row], rank
                )

    def share_across():
        part, paired, out, into = item(ep_count)
        for k in range(1, half):
            gather(k)
            out(k)[...] = combined[...].astype(bf16)
            send(
                out(k),
                into(k),
                back_x_send.at[ep_count, k],
                back_x_recv.at[ep_count, k],
                {"tp": lax.rem(pair + k, half) * 2 + core},
            )
        gather(0)

    def share_finish():
        part, paired, out, into = item(ep_count)
        total = combined[...]
        for k in range(1, half):
            landed(into(k), back_x_recv.at[ep_count, k])
            total = total + into(k)[...].astype(f32)
        channel_out[...] = total.astype(bf16)

    def combine(d):
        source = source_of(d)
        landed(returned.at[source], back_z_recv.at[source])
        add_results(
            lambda columns: returned[source, :, :, columns],
            meta_tp[t],
            source,
        )

    last = ep_count - 1
    pair_count = query.shape[0] // 2

    def expert_item(d):
        all_here(d)
        experts(d)
        to_sibling(d)

    for n in range(8, 14):
        loads[n].wait()
    all_here(ep_count + 1, (0,))
    all_here(ep_count, (0,))
    begin_pair(pair)
    pass_on(ep_count + 1)
    pass_on(ep_count)
    relay(2)
    relay(1)
    come(1)
    branch(early, lambda: come(2))
    for k in range(1, half):
        all_here(ep_count + 1, (k,))
        all_here(ep_count, (k,))
        begin_pair(lax.rem(pair + k, half))
    experts(0)
    relay(3, (0,))
    pass_on(1)
    relay(3, (1,))
    branch(late, lambda: come(2))
    note(None, lambda: spread(arrived.at[:, t, source_of(2)], 2))
    expert_item(1)
    branch(late, send_keys, lambda: lend(1))
    branch(early, lambda: across(1))
    come(3)
    branch(early, send_keys)
    note(None, send_keys)
    pass_on(2)
    expert_item(2)

    branch(late, lambda: across(2))
    branch(early, lambda: lend(2), lambda: finish(1))
    for d in range(1, ep_count):
        landed(kv_all.at[source_of(d)], kv_recv.at[source_of(d)])
    attend_two(0)
    for d in range(3, ep_count):
        if d > 3:
            relay(d)
            come(d)
        pass_on(d)
        expert_item(d)
        across(d)
    branch(late, lambda: finish(2))
    note(late, lambda: lend(1), lambda: across(2), lambda: finish(2))
    note(early, lambda: lend(2), lambda: across(1), lambda: finish(1))
    for n in range(1, pair_count):
        attend_two(n)
    loads[14].wait()
    project()
    to_sibling(ep_count + 1)
    across(ep_count + 1)
    branch(late, lambda: finish(3))
    share()
    to_sibling(ep_count)
    branch(early, lambda: finish(3))
    note(None, lambda: finish(3))
    for d in range(4, ep_count):
        finish(d)
    share_across()
    finish(ep_count + 1)
    for d in (1, 2):
        pl.when(first_of(source_of(d)) != e)(functools.partial(combine, d))
    for d in range(3, ep_count):
        combine(d)
    share_finish()
    for wanted, wait in sends:
        if wanted is None:
            wait()
        else:
            pl.when(wanted)(wait)


def whole(ep_count, tp_count, small, weights):
    queries, key_values, query_gain, key_gain, batch, norm_gain, routes, route_weights = small
    out_weight, gate, up, down, shared_gate, shared_up, shared_down = weights
    local_count = gate.shape[0]
    tok_count, width = batch.shape
    query_rows, wide = key_values.shape
    head_size = query_gain.shape[1]
    heads_here = queries.shape[1] // head_size
    expert_count = local_count * ep_count
    capacity = 3 * tok_count * routes.shape[0] // (2 * expert_count)
    capacity = (capacity + 7) // 8 * 8
    direct = 2 * local_count * capacity <= tok_count
    anywhere = pl.BlockSpec(memory_space=pl.ANY)
    half = tp_count // 2
    dma = pltpu.SemaphoreType.DMA
    block = (local_count, capacity, width)
    spread_block = (local_count, tp_count, ep_count, capacity, width)
    token_block = (tok_count, width)
    mixed = (query_rows // tp_count, width)
    count = ep_count + 2

    def room(*shape):
        return pltpu.VMEM(shape, jnp.bfloat16)

    def wide_room(*shape):
        return pltpu.VMEM(shape, jnp.float32)

    return pl.pallas_call(
        functools.partial(whole_kernel, ep_count, tp_count, direct),
        out_shape=(
            jax.ShapeDtypeStruct(token_block, jnp.bfloat16),
            jax.ShapeDtypeStruct(mixed, jnp.bfloat16),
        ),
        in_specs=[anywhere] * (len(small) + len(weights)),
        out_specs=(pl.BlockSpec(memory_space=pltpu.VMEM),) * 2,
        scratch_shapes=[
            room(*queries.shape),
            room(*key_values.shape),
            wide_room(2, 1, head_size),
            room(*batch.shape),
            wide_room(*norm_gain.shape),
            pltpu.VMEM(routes.shape, jnp.int32),
            wide_room(*route_weights.shape),
            wide_room(4, GRID_W, wide),
            room(heads_here, query_rows, wide),
            room(*((ep_count,) + (block if direct else token_block))),
            room(*spread_block),
            room(tp_count, *token_block),
            room(ep_count, *key_values.shape),
            wide_room(ep_count, 8, tok_count),
            wide_room(tp_count, 8, tok_count),
            room(*out_weight.shape),
            room(*gate.shape),
            room(*up.shape),
            room(*down.shape),
            room(shared_gate.shape[0], 2 * shared_gate.shape[1]),
            room(*shared_down.shape),
            room(query_rows, heads_here // 2 * wide),
            room(*spread_block),
            room(tp_count, *token_block),
            room(tp_count, *mixed),
            room(tp_count, tok_count, shared_down.shape[0]),
            room(tp_count, 2, local_count * capacity, tok_count),
            wide_room(*token_block),
            room(ep_count, *block),
            room(*((1 if direct else ep_count - 1,) + block)),
            room(half, *block),
            room(2, half, *block),
            room(ep_count, half, *block),
            room(ep_count, half - 1, *block),
            room(ep_count, half - 1, *block),
            room(ep_count, *block),
            room(half, *token_block),
            room(half - 1, *token_block),
            room(half - 1, *token_block),
            room(half, *mixed),
            room(half - 1, *mixed),
            room(half - 1, *mixed),
            dma((len(small) + len(weights),)),
            dma((ep_count,)),
            dma((ep_count,)),
            dma((ep_count,)),
            dma((ep_count,)),
            dma((half,)),
            dma((2, half)),
            dma((ep_count, 2)),
            dma((ep_count, 2)),
            dma((ep_count + 1,)),
            dma((ep_count,)),
            dma((half, ep_count + 2)),
            dma((half, ep_count + 2)),
            dma((half, ep_count + 2)),
            dma((half, ep_count + 2)),
            dma((count, half)),
            dma((count, half)),
            dma((count, half)),
            dma((count, half)),
            dma((ep_count,)),
            dma((ep_count,)),
        ],
        compiler_params=pltpu.CompilerParams(
            collective_id=0, has_side_effects=True, vmem_limit_bytes=67043328
        ),
    )(*small, *weights)


def settle_kernel(*refs):
    count = (len(refs) - 1) // 3
    sources, targets, rooms = (refs[n * count : (n + 1) * count] for n in range(3))
    sem = refs[-1]
    moves = []
    for n, (source, room, target) in enumerate(zip(sources, rooms, targets)):
        rows = source.shape[0] // 2
        for c in range(2):
            part = pl.ds(c * rows, rows)
            taken = pltpu.make_async_copy(source.at[part], room.at[part], sem.at[0, n, c])
            given = pltpu.make_async_copy(room.at[part], target.at[part], sem.at[1, n, c])
            taken.start()
            moves.append((taken, given))
    for taken, given in moves:
        taken.wait()
        given.start()
    for taken, given in moves:
        given.wait()


def settle(*arrays):
    anywhere = pl.BlockSpec(memory_space=pl.ANY)
    return pl.pallas_call(
        settle_kernel,
        out_shape=tuple(jax.ShapeDtypeStruct(a.shape, a.dtype) for a in arrays),
        in_specs=[anywhere] * len(arrays),
        out_specs=(anywhere,) * len(arrays),
        scratch_shapes=[pltpu.VMEM(a.shape, a.dtype) for a in arrays]
        + [pltpu.SemaphoreType.DMA((2, len(arrays), 2))],
    )(*arrays)


def body(
    queries,
    key_values,
    query_gain,
    key_gain,
    out_weight,
    second_batch,
    norm_gain,
    routes,
    route_weights,
    expert_gate,
    expert_up,
    expert_down,
    shared_gate,
    shared_up,
    shared_down,
):
    channel_out, mixer_out = whole(
        lax.axis_size("ep"),
        lax.axis_size("tp"),
        (
            queries,
            key_values,
            query_gain[None, :],
            key_gain[None, :],
            second_batch,
            norm_gain[None, :],
            routes.T,
            route_weights.T,
        ),
        (
            out_weight,
            expert_gate,
            expert_up,
            expert_down,
            shared_gate,
            shared_up,
            shared_down,
        ),
    )
    return settle(mixer_out, channel_out)


def solution(mesh):
    placed = (
        P(("grp", "ep"), "tp"),
        P(("grp", "ep"), "tp"),
        P(),
        P(),
        P("tp", None),
        P(("grp", "ep", "tp"), None),
        P(),
        P(("grp", "ep", "tp"), None),
        P(("grp", "ep", "tp"), None),
        P("ep", None, "tp"),
        P("ep", None, "tp"),
        P("ep", "tp", None),
        P(None, "tp"),
        P(None, "tp"),
        P("tp", None),
    )
    return jax.shard_map(
        body,
        mesh=mesh,
        in_specs=placed,
        out_specs=(P(("grp", "ep", "tp"), None), P(("grp", "ep", "tp"), None)),
        check_vma=False,
    )
```

```python
import functools
import math

import jax
import jax.numpy as jnp
from jax import lax
from jax.experimental import pallas as pl
from jax.experimental.pallas import tpu as pltpu
from jax.sharding import PartitionSpec as P

GRID_W = 64


rope_base = 10000.0
norm_eps = 1e-06

MESH = pl.DeviceIdType.MESH


def greet(ep_count, tp_count, e, t):
    barrier = pltpu.get_barrier_semaphore()
    peers = 0
    for d in range(1, ep_count):
        pl.semaphore_signal(
            barrier, inc=1, device_id={"ep": lax.rem(e + d, ep_count)}, device_id_type=MESH
        )
        peers += 1
    pair = t // 2
    core = lax.rem(t, 2)
    for k in range(1, tp_count // 2):
        pl.semaphore_signal(
            barrier,
            inc=1,
            device_id={"tp": lax.rem(pair + k, tp_count // 2) * 2 + core},
            device_id_type=MESH,
        )
        peers += 1
    pl.semaphore_signal(
        barrier, inc=1, device_id={"tp": pair * 2 + 1 - core}, device_id_type=MESH
    )
    peers += 1
    return lambda: pl.semaphore_wait(barrier, peers)


def remote(src, dst, send, recv, device):
    return pltpu.make_async_remote_copy(
        src_ref=src,
        dst_ref=dst,
        send_sem=send,
        recv_sem=recv,
        device_id=device,
        device_id_type=MESH,
    )


def whole_kernel(
    ep_count,
    tp_count,
    direct,
    queries_hbm,
    kv_hbm,
    query_gain_hbm,
    key_gain_hbm,
    batch_hbm,
    norm_gain_hbm,
    routes_hbm,
    route_weights_hbm,
    out_weight_hbm,
    gate_hbm,
    up_hbm,
    down_hbm,
    shared_gate_hbm,
    shared_up_hbm,
    shared_down_hbm,
    channel_out,
    mixed_sum,
    queries,
    kv_in,
    head_gains,
    batch,
    norm_gain,
    routes,
    route_weights,
    tables,
    query,
    tokens,
    arrived,
    normed_all,
    kv_all,
    meta_ep,
    meta_tp,
    out_weight,
    gate,
    up,
    down,
    shared_both,
    shared_down,
    heads_scr,
    routed,
    shared,
    mixed,
    hidden,
    weights_here,
    combined,
    returned,
    onward,
    lent_out,
    lent_in,
    routed_pair,
    routed_out,
    routed_in,
    routed_done,
    shared_pair,
    shared_out,
    shared_in,
    mixed_pair,
    mixed_out,
    mixed_in,
    local_sem,
    kv_send,
    kv_recv,
    meta_send,
    meta_recv,
    lent_send,
    lent_recv,
    r_send,
    r_recv,
    z_send,
    z_recv,
    x_send,
    x_recv,
    d_send,
    d_recv,
    back_d_send,
    back_d_recv,
    back_x_send,
    back_x_recv,
    back_z_send,
    back_z_recv,
):
    e = lax.axis_index("ep")
    t = lax.axis_index("tp")
    half = tp_count // 2
    pair = t // 2
    core = lax.rem(t, 2)
    sibling = {"tp": pair * 2 + 1 - core}
    f32 = jnp.float32
    bf16 = jnp.bfloat16
    head_size = query_gain_hbm.shape[1]
    shared_width = shared_down.shape[0]
    loads = [
        pltpu.make_async_copy(source, target, local_sem.at[n])
        for n, (source, target) in enumerate(
            (
                (batch_hbm, batch),
                (norm_gain_hbm, norm_gain),
                (routes_hbm, routes),
                (route_weights_hbm, route_weights),
                (kv_hbm, kv_in),
                (query_gain_hbm, head_gains.at[0]),
                (key_gain_hbm, head_gains.at[1]),
                (queries_hbm, queries),
                (shared_gate_hbm, shared_both.at[:, :shared_width]),
                (shared_up_hbm, shared_both.at[:, shared_width:]),
                (gate_hbm, gate),
                (up_hbm, up),
                (down_hbm, down),
                (shared_down_hbm, shared_down),
                (out_weight_hbm, out_weight),
            )
        )
    ]
    for copy in loads:
        copy.start()
    greeted = greet(ep_count, tp_count, e, t)

    sends = []

    state = {"start": True, "note": True, "when": None}

    def send(src, dst, send_sem, recv_sem, device):
        copy = remote(src, dst, send_sem, recv_sem, device)
        if state["start"]:
            copy.start()
        if state["note"]:
            sends.append((state["when"], copy.wait_send))

    def branch(when, *steps):
        @pl.when(when)
        def _():
            state["note"] = False
            for step in steps:
                step()
            state["note"] = True

    def note(when, *steps):
        state.update(start=False, when=when)
        for step in steps:
            step()
        state.update(start=True, when=None)

    def send_if(wanted, make):
        @pl.when(wanted)
        def _():
            make().start()

        sends.append((wanted, lambda: make().wait_send()))

    def landed(spot, recv_sem):
        if state["start"]:
            remote(spot, spot, kv_send.at[0], recv_sem, sibling).wait_recv()

    near_side = jnp.minimum(e, ep_count - 1 - e)
    far_way = jnp.where(e < ep_count - 1 - e, 1, -1)

    def source_of(d):
        if d == 0:
            return e
        way = far_way if d % 2 else -far_way
        return jnp.where(
            d <= 2 * near_side, e + way * ((d + 1) // 2), e + far_way * (d - near_side)
        )

    def first_of(rank):
        inner = jnp.where(rank < ep_count - 1 - rank, rank - 1, rank + 1)
        return jnp.where(rank == 0, 1, jnp.where(rank == ep_count - 1, ep_count - 2, inner))

    tok_count, model_width = batch.shape
    local_count, capacity = arrived.shape[0], arrived.shape[3]
    near_count = local_count * capacity
    tile = min(512, model_width)

    def tiles(step, first=0, stop=model_width):
        def run(m, ignored):
            step(pl.ds(pl.multiple_of(m * tile, tile), tile))
            return ignored

        lax.fori_loop(first // tile, stop // tile, run, 0)

    half_width = model_width // 2
    sides = [(c * half_width, (c + 1) * half_width) for c in range(2)]

    def picks_of(meta, rank, ranks=1):
        rows = ranks * near_count
        numbers = lax.broadcasted_iota(jnp.int32, (rows, tok_count), 0)
        expert = (numbers // capacity + rank * local_count).astype(f32)
        place = lax.rem(numbers, capacity).astype(f32)
        earlier = lax.broadcasted_iota(jnp.int32, (tok_count, tok_count), 0)
        later = lax.broadcasted_iota(jnp.int32, (tok_count, tok_count), 1)
        before = jnp.where(earlier < later, 1.0, 0.0).astype(bf16)
        named = [meta[j : j + 1, :] == expert for j in range(2)]
        any_named = sum(jnp.where(match, 1.0, 0.0) for match in named)
        count = jnp.dot(any_named.astype(bf16), before, preferred_element_type=f32)
        picked = jnp.where(count == place, any_named, 0.0)
        weight = sum(jnp.where(match, meta[2 + j : 3 + j, :], 0.0) for j, match in enumerate(named))
        return picked, picked * weight

    def split(value):
        high = value.astype(bf16)
        return high, (value - high.astype(f32)).astype(bf16)

    def place(d, row):
        if d == ep_count:
            return normed_all.at[row]
        if d == ep_count + 1:
            return meta_tp.at[row]
        return arrived.at[:, row, source_of(d)]

    def spread(src, d):
        for k in range(1, half):
            other = lax.rem(pair + k, half)
            send(
                src,
                place(d, t),
                x_send.at[k, d],
                x_recv.at[pair, d],
                {"tp": other * 2 + core},
            )
        send(src, place(d, t), d_send.at[0, d], d_recv.at[pair, d], sibling)

    def pass_on(d):
        for k in range(1, half):
            other = lax.rem(pair + k, half)
            spot = place(d, other * 2 + core)
            landed(spot, x_recv.at[other, d])
            send(spot, spot, d_send.at[k, d], d_recv.at[other, d], sibling)

    def all_here(d, kinds=range(half)):
        for k in kinds:
            other = lax.rem(pair + k, half)
            landed(place(d, other * 2 + 1 - core), d_recv.at[other, d])

    loads[0].wait()
    loads[1].wait()
    norm_rows = math.gcd(tok_count, 16)

    def norm_step(n, ignored):
        rows = pl.ds(pl.multiple_of(n * norm_rows, norm_rows), norm_rows)
        value = batch[rows, :].astype(f32)
        scale = lax.rsqrt(jnp.mean(value * value, axis=-1, keepdims=True) + norm_eps)
        normed_all[t, rows, :] = (value * scale * norm_gain[...]).astype(bf16)
        return ignored

    lax.fori_loop(0, tok_count // norm_rows, norm_step, 0)
    loads[2].wait()
    loads[3].wait()
    meta_tp[t, 0:2, :] = routes[...].astype(f32)
    meta_tp[t, 2:4, :] = route_weights[...]
    greeted()
    spread(normed_all.at[t], ep_count)
    if not direct:
        send_if(
            e < ep_count - 1,
            lambda: remote(
                normed_all.at[t], tokens.at[e], z_send.at[e], z_recv.at[e], {"ep": e + 1}
            ),
        )
        send_if(
            e > 0,
            lambda: remote(
                normed_all.at[t], tokens.at[e], z_send.at[ep_count], z_recv.at[e], {"ep": e - 1}
            ),
        )
    spread(meta_tp.at[t], ep_count + 1)
    if direct:
        picked, ignored_weight = picks_of(meta_tp[t], 0, ep_count)
        picked = picked.astype(bf16)

        def block_step(columns):
            part = jnp.dot(picked, normed_all[t, :, columns], preferred_element_type=f32)
            tokens[:, :, :, columns] = part.reshape(
                ep_count, local_count, capacity, tile
            ).astype(bf16)

        tiles(block_step)
        for d in range(1, ep_count):
            there = lax.rem(e + d, ep_count)
            send(
                tokens.at[there], arrived.at[:, t, e], z_send.at[d], z_recv.at[e], {"ep": there}
            )
    else:
        for d in range(1, ep_count):
            there = lax.rem(e + d, ep_count)
            send(meta_tp.at[t], meta_ep.at[e], meta_send.at[d], meta_recv.at[e], {"ep": there})

    query_rows, wide = query.shape[1], query.shape[2]
    groups = query_rows // GRID_W
    lane = lax.broadcasted_iota(jnp.int32, (GRID_W, wide), 1)
    low = lane < head_size

    def turn_tables():
        in_head = lax.rem(lane, head_size)
        step = lax.rem(in_head // 2, head_size // 4).astype(f32)
        inverse = jnp.exp(step * (-4.0 / head_size * math.log(rope_base)))
        number = lax.broadcasted_iota(jnp.int32, (GRID_W, wide), 0)
        sign = jnp.where(lax.rem(lane, 2) == 0, -1.0, 1.0)
        column_angle = number.astype(f32) * inverse
        tables[0] = jnp.cos(column_angle)
        tables[1] = jnp.sin(column_angle) * sign
        short = tables.shape[1] // 4
        row_angle = (number + e * groups).astype(f32)[:short] * inverse[:short]
        tables[2, :short] = jnp.cos(row_angle)
        tables[3, :short] = jnp.sin(row_angle) * sign[:short]

    def turn(value, group):
        by_row = lax.rem(lane, head_size) < head_size // 2
        cosine = jnp.where(by_row, tables[2, pl.ds(group, 1), :], tables[0])
        sine = jnp.where(by_row, tables[3, pl.ds(group, 1), :], tables[1])
        swapped = jnp.where(
            lax.rem(lane, 2) == 0, pltpu.roll(value, wide - 1, 1), pltpu.roll(value, 1, 1)
        )
        return value * cosine + swapped * sine

    def gain_of(n):
        value = head_gains[n]
        return jnp.concatenate([value] * (wide // head_size), axis=1)

    for n in (4, 5, 6):
        loads[n].wait()
    turn_tables()

    def key_step(group, ignored):
        rows = pl.ds(pl.multiple_of(group * GRID_W, GRID_W), GRID_W)
        value = kv_in[rows, :].astype(f32)
        square = jnp.sum(jnp.where(low, value * value, 0.0), axis=-1, keepdims=True)
        scaled = value * lax.rsqrt(square / head_size + norm_eps) * gain_of(1)
        kv_all[e, rows, :] = jnp.where(low, turn(scaled, group), value).astype(bf16)
        return ignored

    lax.fori_loop(0, groups, key_step, 0)
    loads[7].wait()

    def query_step(group, ignored):
        rows = pl.ds(pl.multiple_of(group * GRID_W, GRID_W), GRID_W)
        for n in range(query.shape[0] // 2):
            value = queries[rows, n * wide : (n + 1) * wide].astype(f32)
            square = value * value
            sums = [
                jnp.sum(jnp.where(side, square, 0.0), axis=-1, keepdims=True)
                for side in (low, jnp.logical_not(low))
            ]
            scales = [lax.rsqrt(total / head_size + norm_eps) for total in sums]
            scaled = value * jnp.where(low, scales[0], scales[1]) * gain_of(0)
            turned = turn(scaled, group) * head_size ** (-0.5)
            query[2 * n, rows, :] = jnp.where(low, turned, 0.0).astype(bf16)
            query[2 * n + 1, rows, :] = jnp.where(
                low, pltpu.roll(turned, wide // 2, 1), 0.0
            ).astype(bf16)
        return ignored

    lax.fori_loop(0, groups, query_step, 0)

    early = near_side > 0
    late = jnp.logical_not(early)

    def pick_into(source, rank, target, first=0, stop=model_width):
        picked, ignored_weight = picks_of(meta_ep[source], rank)
        picked = picked.astype(bf16)

        def pick_step(columns):
            part = jnp.dot(picked, tokens[source, :, columns], preferred_element_type=f32)
            target(columns, part.reshape(local_count, capacity, tile).astype(bf16))

        tiles(pick_step, first, stop)

    def relay(d, parts=(0, 1)):
        if direct:
            return
        source = source_of(d)
        target = jnp.where(source > e, e - 1, e + 1)
        to_end = jnp.logical_or(target == 0, target == ep_count - 1)
        whole_rows = jnp.logical_and(early, jnp.logical_not(to_end))
        picked_rows = jnp.logical_and(early, to_end)

        @pl.when(early)
        def _():
            if d <= 2:
                landed(tokens.at[source], z_recv.at[source])
            if 0 in parts:
                landed(meta_ep.at[source], meta_recv.at[source])

        for c in parts:
            first, stop = sides[c]
            if d > 2:

                @pl.when(early)
                def _():
                    landed(tokens.at[source, :, first:stop], r_recv.at[source, c])

            def rows_copy(c=c, first=first, stop=stop):
                spot = tokens.at[source, :, first:stop]
                return remote(
                    spot, spot, r_send.at[source, c], r_recv.at[source, c], {"ep": target}
                )

            def slots_copy(c=c, first=first, stop=stop):
                return remote(
                    onward.at[d - 1, :, :, first:stop],
                    arrived.at[:, t, source, :, first:stop],
                    r_send.at[source, c],
                    r_recv.at[source, c],
                    {"ep": target},
                )

            send_if(whole_rows, rows_copy)

            @pl.when(picked_rows)
            def _():
                def put(columns, value):
                    onward[d - 1, :, :, columns] = value

                pick_into(source, target, put, first, stop)

            send_if(picked_rows, slots_copy)

    def pick_here(d):
        source = source_of(d)

        def put(columns, value):
            arrived[:, t, source, :, columns] = value

        pick_into(source, e, put)

    def come(d):
        source = source_of(d)
        spot = arrived.at[:, t, source]
        if direct:
            landed(spot, z_recv.at[source])
        elif d == 1:

            @pl.when(late)
            def _():
                landed(tokens.at[source], z_recv.at[source])
                landed(meta_ep.at[source], meta_recv.at[source])

            pick_here(d)
        else:

            @pl.when(late)
            def _():
                for c, (first, stop) in enumerate(sides):
                    landed(spot.at[:, :, first:stop], r_recv.at[source, c])
                landed(meta_ep.at[source], meta_recv.at[source])

            @pl.when(early)
            def _():
                pick_here(d)

        spread(spot, d)

    def send_keys():
        for d in range(1, ep_count):
            there = lax.rem(e + d, ep_count)
            send(kv_all.at[e], kv_all.at[e], kv_send.at[d], kv_recv.at[e], {"ep": there})

    def attend(h):
        def step(b, carried):
            top_now, total_now, acc_now = carried
            block = kv_all[b]
            scores = lax.dot_general(
                query[h], block, (((1,), (1,)), ((), ())), preferred_element_type=f32
            )
            top_new = jnp.maximum(top_now, jnp.max(scores, axis=-1, keepdims=True))
            shrink = jnp.exp(top_now - top_new)
            exps = jnp.exp(scores - top_new)
            total_new = total_now * shrink + jnp.sum(exps, axis=-1, keepdims=True)
            acc_new = acc_now * shrink + jnp.dot(
                exps.astype(bf16), block, preferred_element_type=f32
            )
            return (top_new, total_new, acc_new)

        start = (
            jnp.full((query_rows, 1), -1e30, f32),
            jnp.zeros((query_rows, 1), f32),
            jnp.zeros((query_rows, wide), f32),
        )
        top, total, acc = lax.fori_loop(0, ep_count, step, start)
        return acc / total

    def attend_two(n):
        low = pltpu.roll(attend(2 * n), wide // 2, 1)
        high = attend(2 * n + 1)
        lane = lax.broadcasted_iota(jnp.int32, low.shape, 1)
        heads_scr[:, n * wide : (n + 1) * wide] = jnp.where(lane < wide // 2, low, high).astype(
            bf16
        )

    def project():
        def step(n, ignored):
            columns = pl.ds(pl.multiple_of(n * tile, tile), tile)
            part = jnp.dot(heads_scr[...], out_weight[:, columns], preferred_element_type=f32)
            mixed[:, :, columns] = part.astype(bf16).reshape(
                tp_count, query_rows // tp_count, tile
            )
            return ignored

        lax.fori_loop(0, model_width // tile, step, 0)

    def begin(row):
        both_parts = jnp.dot(normed_all[row], shared_both[...], preferred_element_type=f32)
        gate_part = both_parts[:, :shared_width]
        up_part = both_parts[:, shared_width:]
        hidden[row] = (gate_part / (1.0 + jnp.exp(-gate_part)) * up_part).astype(bf16)
        picked, weight = picks_of(meta_tp[row], e)
        for n, part in enumerate(split(weight)):
            weights_here[row, n] = part
        picked = picked.astype(bf16)

        def columns_step(columns):
            part = jnp.dot(picked, normed_all[row, :, columns], preferred_element_type=f32)
            arrived[:, row, e, :, columns] = part.reshape(local_count, capacity, tile).astype(
                bf16
            )

        tiles(columns_step)

    def begin_pair(which):
        def step(n, ignored):
            begin(which * 2 + n)
            return ignored

        lax.fori_loop(0, 2, step, 0)

    def share():
        def step(row, ignored):
            def columns_step(columns):
                results = routed[:, row, e, :, columns]
                if capacity % 16:
                    results = results.astype(f32)
                results = results.reshape(near_count, tile).astype(bf16)
                part = jnp.dot(
                    hidden[row], shared_down[:, columns], preferred_element_type=f32
                )
                part = part + lax.dot_general(
                    weights_here[row].reshape(2 * near_count, tok_count),
                    jnp.concatenate([results, results], axis=0),
                    (((0,), (0,)), ((), ())),
                    preferred_element_type=f32,
                )
                shared[row, :, columns] = part.astype(bf16)

            tiles(columns_step)
            return ignored

        lax.fori_loop(0, tp_count, step, 0)

    def experts(d):
        source = source_of(d)

        def step(n, ignored):
            rows = arrived[n, :, source]
            if capacity % 16:
                rows = rows.astype(f32)
            rows = rows.reshape(tp_count * capacity, model_width).astype(bf16)
            gate_part = jnp.dot(rows, gate[n], preferred_element_type=f32)
            up_part = jnp.dot(rows, up[n], preferred_element_type=f32)
            hidden = (gate_part / (1.0 + jnp.exp(-gate_part)) * up_part).astype(bf16)

            def columns_step(m, inner):
                columns = pl.ds(pl.multiple_of(m * tile, tile), tile)
                part = jnp.dot(hidden, down[n, :, columns], preferred_element_type=f32)
                if capacity % 16:
                    part = part.reshape(tp_count, capacity, tile).astype(bf16)
                else:
                    part = part.astype(bf16).reshape(tp_count, capacity, tile)
                routed[n, :, source, :, columns] = part
                return inner

            lax.fori_loop(0, model_width // tile, columns_step, 0)
            return ignored

        lax.fori_loop(0, local_count, step, 0)

    def item(d):
        if d < ep_count:
            source = source_of(d)
            return (
                lambda row: routed.at[:, row, source],
                lambda k: routed_pair.at[d, k],
                lambda k: routed_out.at[d, k - 1],
                lambda k: routed_in.at[d, k - 1],
            )
        if d == ep_count:
            return (
                lambda row: shared.at[row],
                lambda k: shared_pair.at[k],
                lambda k: shared_out.at[k - 1],
                lambda k: shared_in.at[k - 1],
            )
        return (
            lambda row: mixed.at[row],
            lambda k: mixed_pair.at[k],
            lambda k: mixed_out.at[k - 1],
            lambda k: mixed_in.at[k - 1],
        )

    def to_sibling(d):
        part, paired, out, into = item(d)
        for k in list(range(1, half)) + [0]:
            other = lax.rem(pair + k, half)
            send(
                part(other * 2 + 1 - core),
                paired(k),
                back_d_send.at[d, k],
                back_d_recv.at[d, k],
                sibling,
            )

    def both(d, k):
        part, paired, out, into = item(d)
        spot = paired(k)
        landed(spot, back_d_recv.at[d, k])
        mine = part(lax.rem(pair + k, half) * 2 + core)
        return mine[...].astype(f32) + spot[...].astype(f32)

    def across(d):
        part, paired, out, into = item(d)
        for k in range(1, half):
            other = lax.rem(pair + k, half)
            if state["start"]:
                out(k)[...] = both(d, k).astype(bf16)
            send(
                out(k),
                into(k),
                back_x_send.at[d, k],
                back_x_recv.at[d, k],
                {"tp": other * 2 + core},
            )

    def finish(d):
        part, paired, out, into = item(d)
        if state["start"]:
            total = both(d, 0)
            for k in range(1, half):
                spot = into(k)
                landed(spot, back_x_recv.at[d, k])
                total = total + spot[...].astype(f32)
            if d > ep_count:
                mixed_sum[...] = total.astype(bf16)
                return
            routed_done[d] = total.astype(bf16)
        send(
            routed_done.at[d],
            returned.at[e],
            back_z_send.at[d],
            back_z_recv.at[e],
            {"ep": source_of(d)},
        )

    def lend(d):
        home = source_of(d)
        side = jnp.where(home > e, 0, 1)
        for k in list(range(1, half)) + [0]:
            if state["start"]:
                lent_out[k] = both(d, k).astype(bf16)
            send(
                lent_out.at[k],
                lent_in.at[side, k],
                lent_send.at[k],
                lent_recv.at[side, k],
                {"ep": home},
            )

    def add_results(results_of, meta, rank):
        ignored_pick, weight = picks_of(meta, rank)
        weights = jnp.concatenate(split(weight), axis=0)

        def columns_step(columns):
            results = results_of(columns)
            if capacity % 16:
                results = results.astype(f32)
            results = results.reshape(near_count, tile).astype(bf16)
            part = lax.dot_general(
                weights,
                jnp.concatenate([results, results], axis=0),
                (((0,), (0,)), ((), ())),
                preferred_element_type=f32,
            )
            combined[:, columns] = combined[:, columns] + part

        tiles(columns_step)

    def gather(k):
        combined[...] = both(ep_count, k)
        row = lax.rem(pair + k, half) * 2 + core
        below = jnp.logical_and(e > 0, first_of(e - 1) == e)
        above = jnp.logical_and(e < ep_count - 1, first_of(e + 1) == e)
        for side, there, rank in ((0, below, e - 1), (1, above, e + 1)):

            @pl.when(there)
            def _():
                landed(lent_in.at[side, k], lent_recv.at[side, k])
                add_results(
                    lambda columns: lent_in[side, k, :, :, columns], meta_tp[row], rank
                )

    def share_across():
        part, paired, out, into = item(ep_count)
        for k in range(1, half):
            gather(k)
            out(k)[...] = combined[...].astype(bf16)
            send(
                out(k),
                into(k),
                back_x_send.at[ep_count, k],
                back_x_recv.at[ep_count, k],
                {"tp": lax.rem(pair + k, half) * 2 + core},
            )
        gather(0)

    def share_finish():
        part, paired, out, into = item(ep_count)
        total = combined[...]
        for k in range(1, half):
            landed(into(k), back_x_recv.at[ep_count, k])
            total = total + into(k)[...].astype(f32)
        channel_out[...] = total.astype(bf16)

    def combine(d):
        source = source_of(d)
        landed(returned.at[source], back_z_recv.at[source])
        add_results(
            lambda columns: returned[source, :, :, columns],
            meta_tp[t],
            source,
        )

    last = ep_count - 1
    pair_count = query.shape[0] // 2

    def expert_item(d):
        all_here(d)
        experts(d)
        to_sibling(d)

    for n in range(8, 14):
        loads[n].wait()
    all_here(ep_count + 1, (0,))
    all_here(ep_count, (0,))
    begin_pair(pair)
    pass_on(ep_count + 1)
    pass_on(ep_count)
    relay(2)
    relay(1)
    come(1)
    branch(early, lambda: come(2))
    for k in range(1, half):
        all_here(ep_count + 1, (k,))
        all_here(ep_count, (k,))
        begin_pair(lax.rem(pair + k, half))
    experts(0)
    relay(3, (0,))
    pass_on(1)
    relay(3, (1,))
    branch(late, lambda: come(2))
    note(None, lambda: spread(arrived.at[:, t, source_of(2)], 2))
    expert_item(1)
    branch(late, send_keys, lambda: lend(1))
    branch(early, lambda: across(1))
    come(3)
    branch(early, send_keys)
    note(None, send_keys)
    pass_on(2)
    expert_item(2)

    branch(late, lambda: across(2))
    branch(early, lambda: lend(2), lambda: finish(1))
    for d in range(1, ep_count):
        landed(kv_all.at[source_of(d)], kv_recv.at[source_of(d)])
    attend_two(0)
    for d in range(3, ep_count):
        if d > 3:
            relay(d)
            come(d)
        pass_on(d)
        expert_item(d)
        across(d)
    branch(late, lambda: finish(2))
    note(late, lambda: lend(1), lambda: across(2), lambda: finish(2))
    note(early, lambda: lend(2), lambda: across(1), lambda: finish(1))
    for n in range(1, pair_count):
        attend_two(n)
    loads[14].wait()
    project()
    to_sibling(ep_count + 1)
    across(ep_count + 1)
    branch(late, lambda: finish(3))
    share()
    to_sibling(ep_count)
    branch(early, lambda: finish(3))
    note(None, lambda: finish(3))
    for d in range(4, ep_count):
        finish(d)
    share_across()
    finish(ep_count + 1)
    for d in (1, 2):
        pl.when(first_of(source_of(d)) != e)(functools.partial(combine, d))
    for d in range(3, ep_count):
        combine(d)
    share_finish()
    for wanted, wait in sends:
        if wanted is None:
            wait()
        else:
            pl.when(wanted)(wait)


def whole(ep_count, tp_count, small, weights):
    queries, key_values, query_gain, key_gain, batch, norm_gain, routes, route_weights = small
    out_weight, gate, up, down, shared_gate, shared_up, shared_down = weights
    local_count = gate.shape[0]
    tok_count, width = batch.shape
    query_rows, wide = key_values.shape
    head_size = query_gain.shape[1]
    heads_here = queries.shape[1] // head_size
    expert_count = local_count * ep_count
    capacity = 3 * tok_count * routes.shape[0] // (2 * expert_count)
    capacity = (capacity + 7) // 8 * 8
    direct = 2 * local_count * capacity <= tok_count
    anywhere = pl.BlockSpec(memory_space=pl.ANY)
    half = tp_count // 2
    dma = pltpu.SemaphoreType.DMA
    block = (local_count, capacity, width)
    spread_block = (local_count, tp_count, ep_count, capacity, width)
    token_block = (tok_count, width)
    mixed = (query_rows // tp_count, width)
    count = ep_count + 2

    def room(*shape):
        return pltpu.VMEM(shape, jnp.bfloat16)

    def wide_room(*shape):
        return pltpu.VMEM(shape, jnp.float32)

    return pl.pallas_call(
        functools.partial(whole_kernel, ep_count, tp_count, direct),
        out_shape=(
            jax.ShapeDtypeStruct(token_block, jnp.bfloat16),
            jax.ShapeDtypeStruct(mixed, jnp.bfloat16),
        ),
        in_specs=[anywhere] * (len(small) + len(weights)),
        out_specs=(pl.BlockSpec(memory_space=pltpu.VMEM),) * 2,
        scratch_shapes=[
            room(*queries.shape),
            room(*key_values.shape),
            wide_room(2, 1, head_size),
            room(*batch.shape),
            wide_room(*norm_gain.shape),
            pltpu.VMEM(routes.shape, jnp.int32),
            wide_room(*route_weights.shape),
            wide_room(4, GRID_W, wide),
            room(heads_here, query_rows, wide),
            room(*((ep_count,) + (block if direct else token_block))),
            room(*spread_block),
            room(tp_count, *token_block),
            room(ep_count, *key_values.shape),
            wide_room(ep_count, 8, tok_count),
            wide_room(tp_count, 8, tok_count),
            room(*out_weight.shape),
            room(*gate.shape),
            room(*up.shape),
            room(*down.shape),
            room(shared_gate.shape[0], 2 * shared_gate.shape[1]),
            room(*shared_down.shape),
            room(query_rows, heads_here // 2 * wide),
            room(*spread_block),
            room(tp_count, *token_block),
            room(tp_count, *mixed),
            room(tp_count, tok_count, shared_down.shape[0]),
            room(tp_count, 2, local_count * capacity, tok_count),
            wide_room(*token_block),
            room(ep_count, *block),
            room(*((1 if direct else ep_count - 1,) + block)),
            room(half, *block),
            room(2, half, *block),
            room(ep_count, half, *block),
            room(ep_count, half - 1, *block),
            room(ep_count, half - 1, *block),
            room(ep_count, *block),
            room(half, *token_block),
            room(half - 1, *token_block),
            room(half - 1, *token_block),
            room(half, *mixed),
            room(half - 1, *mixed),
            room(half - 1, *mixed),
            dma((len(small) + len(weights),)),
            dma((ep_count,)),
            dma((ep_count,)),
            dma((ep_count,)),
            dma((ep_count,)),
            dma((half,)),
            dma((2, half)),
            dma((ep_count, 2)),
            dma((ep_count, 2)),
            dma((ep_count + 1,)),
            dma((ep_count,)),
            dma((half, ep_count + 2)),
            dma((half, ep_count + 2)),
            dma((half, ep_count + 2)),
            dma((half, ep_count + 2)),
            dma((count, half)),
            dma((count, half)),
            dma((count, half)),
            dma((count, half)),
            dma((ep_count,)),
            dma((ep_count,)),
        ],
        compiler_params=pltpu.CompilerParams(
            collective_id=0, has_side_effects=True, vmem_limit_bytes=67043328
        ),
    )(*small, *weights)


def settle_kernel(*refs):
    count = (len(refs) - 1) // 3
    sources, targets, rooms = (refs[n * count : (n + 1) * count] for n in range(3))
    sem = refs[-1]
    moves = []
    for n, (source, room, target) in enumerate(zip(sources, rooms, targets)):
        rows = source.shape[0] // 2
        for c in range(2):
            part = pl.ds(c * rows, rows)
            taken = pltpu.make_async_copy(source.at[part], room.at[part], sem.at[0, n, c])
            given = pltpu.make_async_copy(room.at[part], target.at[part], sem.at[1, n, c])
            taken.start()
            moves.append((taken, given))
    for taken, given in moves:
        taken.wait()
        given.start()
    for taken, given in moves:
        given.wait()


def settle(*arrays):
    anywhere = pl.BlockSpec(memory_space=pl.ANY)
    return pl.pallas_call(
        settle_kernel,
        out_shape=tuple(jax.ShapeDtypeStruct(a.shape, a.dtype) for a in arrays),
        in_specs=[anywhere] * len(arrays),
        out_specs=(anywhere,) * len(arrays),
        scratch_shapes=[pltpu.VMEM(a.shape, a.dtype) for a in arrays]
        + [pltpu.SemaphoreType.DMA((2, len(arrays), 2))],
    )(*arrays)


def body(
    queries,
    key_values,
    query_gain,
    key_gain,
    out_weight,
    second_batch,
    norm_gain,
    routes,
    route_weights,
    expert_gate,
    expert_up,
    expert_down,
    shared_gate,
    shared_up,
    shared_down,
):
    channel_out, mixer_out = whole(
        lax.axis_size("ep"),
        lax.axis_size("tp"),
        (
            queries,
            key_values,
            query_gain[None, :],
            key_gain[None, :],
            second_batch,
            norm_gain[None, :],
            routes.T,
            route_weights.T,
        ),
        (
            out_weight,
            expert_gate,
            expert_up,
            expert_down,
            shared_gate,
            shared_up,
            shared_down,
        ),
    )
    return settle(mixer_out, channel_out)


def solution(mesh):
    placed = (
        P(("grp", "ep"), "tp"),
        P(("grp", "ep"), "tp"),
        P(),
        P(),
        P("tp", None),
        P(("grp", "ep", "tp"), None),
        P(),
        P(("grp", "ep", "tp"), None),
        P(("grp", "ep", "tp"), None),
        P("ep", None, "tp"),
        P("ep", None, "tp"),
        P("ep", "tp", None),
        P(None, "tp"),
        P(None, "tp"),
        P("tp", None),
    )
    return jax.shard_map(
        body,
        mesh=mesh,
        in_specs=placed,
        out_specs=(P(("grp", "ep", "tp"), None), P(("grp", "ep", "tp"), None)),
        check_vma=False,
    )
```
